512 devices in a mesh: sp: 64 (over z, y), tp: 8 (over x, core).
Axes of the slice: x: 4, y: 4, z: 16, core: 2. Of those that a mesh axis runs over, the one named last changes fastest.
Arguments:
- acceptor_signal: bfloat16 [8192, 1024], P('sp', 'tp'), may hold values from -6 to 6
- address_entries: bfloat16 [8192, 1024], P('sp', 'tp'), may hold values from -6 to 6
- payload_entries: bfloat16 [8192, 1024], P('sp', 'tp'), may hold values from -6 to 6
- fading_logits: float32 [8192, 1024], P('sp', 'tp'), may hold values from -12 to -2
- learning_rate_logits: float32 [8192, 1024], P('sp', 'tp'), may hold values from -10 to 4
- exit_switch_entries: bfloat16 [8192, 1024], P('sp', 'tp'), may hold values from -6 to 6
- extra_reward_weights: float32 [1024], P('tp'), may hold values from -0.3 to 0.3
- subspace_rescale_weights: float32 [1024], P('tp'), may hold values from 0.1 to 1.9
- timemix_exit_weights: bfloat16 [1024, 2048], P('tp'), may hold values from -0.1875 to 0.1875
- skip_stream_arriving: bfloat16 [8192, 2048], P(('sp', 'tp')), may hold values from -6 to 6
- pointwise_block_scaling: float32 [2048], replicated, may hold values from 0.1 to 1.9
- switch_projection: bfloat16 [2048, 5632], P('sp', 'tp'), may hold values from -0.125 to 0.125
- widening_projection: bfloat16 [2048, 5632], P('sp', 'tp'), may hold values from -0.125 to 0.125
- switch_filter_coefficients: float32 [3, 5632], P(None, 'tp'), may hold values from -3.5 to 3.5
- narrowing_projection: bfloat16 [5632, 2048], P('tp', 'sp'), may hold values from -0.078125 to 0.078125
Outputs:
- layer_out: bfloat16 [8192, 2048], P(('sp', 'tp'))
The draws below stay inside these ranges and needn't reach their ends.
All inputs are finite; a program needn't handle non-finite values.
Results may differ from the reference program's by a relative error of at most 0.019.
Values may be sent and summed in bfloat16 or wider, within the bound.
A program may use at most 64 MiB of HBM per device.

```python
import jax
import jax.numpy as jnp
from jax import lax

D = 2048
HEADS = 16
SUBSPACE_WIDTH = 64
FF = 5632
TAPS = 3
TOK_DEV = 128
TOKENS = 8192
TIMEMIX_FEATURES = 1024
N_TP = 8


def head_kinds(key):
    drawn = jax.random.randint(jax.random.fold_in(key, 11), (HEADS,), 0, 10)
    slow = drawn < 5
    return jnp.repeat(slow, SUBSPACE_WIDTH)


def draw_fading_logits(key, part):
    slow = head_kinds(key)
    slow_base = 0.3 - jnp.log(TOKENS * 1.0)
    base = jnp.where(slow, slow_base, -3.4).astype(jnp.float32)
    offsets = jax.random.uniform(jax.random.fold_in(key, 21), (TOKENS // TOK_DEV, HEADS * SUBSPACE_WIDTH), jnp.float32, -0.7, 0.7)
    offsets = jnp.repeat(offsets, TOK_DEV, axis=0)
    noise = 0.3 * jax.random.normal(jax.random.fold_in(key, 31), (TOKENS, HEADS * SUBSPACE_WIDTH), jnp.float32)
    return jnp.clip(base[None, :] + offsets + noise, -12.0, -2.0)


def draw_learning_rate_logits(key, part):
    slow = head_kinds(key)
    slow_base = -1.0 - jnp.log(TOKENS / 64.0)
    base = jnp.where(slow, slow_base, 0.0).astype(jnp.float32)
    spread = jnp.where(slow, 0.7, 1.0).astype(jnp.float32)
    noise = jax.random.normal(jax.random.fold_in(key, 41), (TOKENS, HEADS * SUBSPACE_WIDTH), jnp.float32)
    return jnp.clip(base[None, :] + spread[None, :] * noise, -10.0, 4.0)


def block_levels(key, shape, pieces, least, top_value):
    def one(dim, shards_of):
        heights = jax.random.uniform(jax.random.fold_in(jax.random.fold_in(key, 6), dim), (shards_of,), jnp.float32, least / len(pieces), top_value / len(pieces))
        return jnp.repeat(jnp.exp(heights), shape[dim] // shards_of).reshape((-1,) + (1,) * (len(shape) - dim - 1))

    level = one(*pieces[0])
    for cut in pieces[1:]:
        level = level * one(*cut)
    return level


def gaussian(stream_key, dims, scale, reach, shards=(), held_as=jnp.bfloat16):
    values = scale * jax.random.normal(stream_key, dims, jnp.float32)
    if shards:
        values = values * block_levels(stream_key, dims, shards, -0.22, 0.18)
    return jnp.clip(values, -reach, reach).astype(held_as)


def setup_inputs(seed: int = 0) -> dict:
    streams_of = jax.random.split(jax.random.key(seed), 16)
    acceptor_signal = gaussian(streams_of[0], (TOKENS, TIMEMIX_FEATURES), 1.0, 6.0, ((0, 64), (1, 8)))
    address_entries = gaussian(streams_of[1], (TOKENS, TIMEMIX_FEATURES), 1.0, 6.0, ((0, 64), (1, 8)))
    payload_entries = gaussian(streams_of[2], (TOKENS, TIMEMIX_FEATURES), 1.0, 6.0, ((0, 64), (1, 8)))
    fading_logits = draw_fading_logits(jax.random.fold_in(streams_of[15], 71), 0)
    learning_rate_logits = draw_learning_rate_logits(jax.random.fold_in(streams_of[15], 71), 0)
    exit_switch_entries = gaussian(streams_of[5], (TOKENS, TIMEMIX_FEATURES), 1.0, 6.0, ((0, 64), (1, 8)))
    extra_reward_weights = gaussian(streams_of[6], (TIMEMIX_FEATURES,), 0.05, 0.3, ((0, 8),), jnp.float32)
    subspace_rescale_weights = jnp.clip(1.0 + 0.18 * jax.random.normal(streams_of[7], (TIMEMIX_FEATURES,), jnp.float32), 0.1, 1.9)
    timemix_exit_weights = gaussian(streams_of[8], (TIMEMIX_FEATURES, D), TIMEMIX_FEATURES ** -0.5, 0.1875, ((0, 8),))
    skip_stream_arriving = gaussian(streams_of[9], (TOKENS, D), 1.0, 6.0, ((0, 512),))
    pointwise_block_scaling = jnp.clip(1.0 + 0.18 * jax.random.normal(streams_of[10], (D,), jnp.float32), 0.1, 1.9)
    switch_projection = gaussian(streams_of[11], (D, FF), D ** -0.5, 0.125, ((0, 64), (1, 8)))
    widening_projection = gaussian(streams_of[12], (D, FF), D ** -0.5, 0.125, ((0, 64), (1, 8)))
    switch_filter_coefficients = gaussian(streams_of[13], (TAPS, FF), TAPS ** -0.5, 3.5, ((1, 8),), jnp.float32)
    narrowing_projection = gaussian(streams_of[14], (FF, D), FF ** -0.5, 0.078125, ((0, 8), (1, 64)))
    return dict(acceptor_signal=acceptor_signal, address_entries=address_entries, payload_entries=payload_entries, fading_logits=fading_logits, learning_rate_logits=learning_rate_logits, exit_switch_entries=exit_switch_entries, extra_reward_weights=extra_reward_weights, subspace_rescale_weights=subspace_rescale_weights, timemix_exit_weights=timemix_exit_weights, skip_stream_arriving=skip_stream_arriving, pointwise_block_scaling=pointwise_block_scaling, switch_projection=switch_projection, widening_projection=widening_projection, switch_filter_coefficients=switch_filter_coefficients, narrowing_projection=narrowing_projection)


group_eps = 0.00064
norm_eps = 1e-06
highest = lax.Precision.HIGHEST

def by_heads(array):
    return array.astype(jnp.float32).reshape(array.shape[0], -1, SUBSPACE_WIDTH)

def mechanism_inputs(acceptor_signal, address_entries, payload_entries, fading_logits, learning_rate_logits):
    acceptor_entries = by_heads(acceptor_signal)
    address_mapped = by_heads(address_entries)
    payload_mapped = by_heads(payload_entries)
    log_rate = -jax.nn.softplus(-fading_logits) - 0.5
    fading = by_heads(jnp.exp(-jnp.exp(log_rate)))
    erase_rate = by_heads(jax.nn.sigmoid(learning_rate_logits))
    length = jnp.sqrt(lax.optimization_barrier(jnp.sum(address_mapped * address_mapped, axis=-1, keepdims=True)))
    unit_key = address_mapped / jnp.maximum(length, 1.0)
    return (acceptor_entries, address_mapped, payload_mapped, fading, -unit_key, unit_key * erase_rate)

def subspace_outcomes(acceptor_entries, address_mapped, payload_mapped, closing_memory, subspace_rescale_weights, extra_reward_weights, exit_switch_entries):
    centred = closing_memory - lax.optimization_barrier(jnp.mean(closing_memory, axis=-1, keepdims=True))
    rescaled_arguments = centred * lax.rsqrt(lax.optimization_barrier(jnp.mean(centred * centred, axis=-1, keepdims=True)) + group_eps)
    scaling_fetch = subspace_rescale_weights.reshape(-1, SUBSPACE_WIDTH)
    extra_reward_fetch = extra_reward_weights.reshape(-1, SUBSPACE_WIDTH)
    present_extra_reward = lax.optimization_barrier(jnp.sum(acceptor_entries * address_mapped * extra_reward_fetch, axis=-1, keepdims=True)) * payload_mapped
    timemix_product = rescaled_arguments * scaling_fetch + present_extra_reward
    timemix_product = timemix_product.reshape(timemix_product.shape[0], -1) * exit_switch_entries.astype(jnp.float32)
    return timemix_product.astype(jnp.bfloat16)

def token_step(state, sublevel_arguments):
    acceptor_entries, address_mapped, payload_mapped, fading, erase_dir, erase_amt = sublevel_arguments
    along = jnp.einsum('hij,hj->hi', state, erase_dir, precision=highest)
    state = state * fading[:, None, :] + along[:, :, None] * erase_amt[:, None, :] + payload_mapped[:, :, None] * address_mapped[:, None, :]
    return (state, jnp.einsum('hij,hj->hi', state, acceptor_entries, precision=highest))

def grouped_product(left, right, groups):
    width = left.shape[1] // groups
    total = jnp.zeros((left.shape[0], right.shape[1]), jnp.float32)
    for group in range(groups):
        part = jnp.dot(left[:, group * width:(group + 1) * width], right[group * width:(group + 1) * width], preferred_element_type=jnp.float32)
        rounded = lax.optimization_barrier(part.astype(jnp.bfloat16))
        total = total + rounded.astype(jnp.float32)
    return total

def reference(acceptor_signal, address_entries, payload_entries, fading_logits, learning_rate_logits, exit_switch_entries, extra_reward_weights, subspace_rescale_weights, timemix_exit_weights, skip_stream_arriving, pointwise_block_scaling, switch_projection, widening_projection, switch_filter_coefficients, narrowing_projection):
    sublevel_arguments = mechanism_inputs(acceptor_signal, address_entries, payload_entries, fading_logits, learning_rate_logits)
    head_count = sublevel_arguments[0].shape[1]
    initial = jnp.zeros((head_count, SUBSPACE_WIDTH, SUBSPACE_WIDTH), jnp.float32)
    _, closing_memory = lax.scan(token_step, initial, sublevel_arguments)
    timemix_product = subspace_outcomes(sublevel_arguments[0], sublevel_arguments[1], sublevel_arguments[2], closing_memory, subspace_rescale_weights, extra_reward_weights, exit_switch_entries)
    attended = grouped_product(timemix_product, timemix_exit_weights, N_TP)
    hidden_res = skip_stream_arriving.astype(jnp.float32) + attended
    rescaled_arguments = hidden_res * lax.rsqrt(lax.optimization_barrier(jnp.mean(hidden_res * hidden_res, axis=-1, keepdims=True)) + norm_eps) * pointwise_block_scaling
    rescaled_arguments = rescaled_arguments.astype(jnp.bfloat16)
    gate_pre = jnp.dot(rescaled_arguments, switch_projection, preferred_element_type=jnp.float32).astype(jnp.bfloat16)
    up_part = jnp.dot(rescaled_arguments, widening_projection, preferred_element_type=jnp.float32).astype(jnp.bfloat16)
    taps = switch_filter_coefficients.shape[0]
    padded = jnp.pad(gate_pre.astype(jnp.float32), ((taps - 1, 0), (0, 0)))
    length = gate_pre.shape[0]
    conv_out = jnp.zeros(gate_pre.shape, jnp.float32)
    for tap in range(taps):
        conv_out = conv_out + switch_filter_coefficients[tap] * padded[tap:tap + length]
    hidden = (jax.nn.silu(conv_out) * up_part.astype(jnp.float32)).astype(jnp.bfloat16)
    projected = grouped_product(hidden, narrowing_projection, N_TP)
    return (hidden_res + projected).astype(jnp.bfloat16)
```

```python
import functools

import jax
import jax.numpy as jnp
from jax import lax
from jax.experimental import pallas as pl
from jax.experimental.pallas import tpu as pltpu
from jax.sharding import Mesh
from jax.sharding import PartitionSpec as P

WIDTH = 64
SP = ("sp_0", "sp_1")
SP_TP = ("sp_0", "sp_1", "tp")
COLUMNS = 4
MESH = pl.DeviceIdType.MESH

group_eps = 0.00064
norm_eps = 1e-06
f32 = jnp.float32
bf16 = jnp.bfloat16

NN = (((1,), (0,)), ((), ()))
NT = (((1,), (1,)), ((), ()))
TN = (((0,), (0,)), ((), ()))


def exact(a, b, dims=NN):
    return lax.dot_general(
        a, b, dims, precision=lax.Precision.HIGHEST, preferred_element_type=f32
    )


def plain(a, b, dims=NN):
    return lax.dot_general(a, b, dims, preferred_element_type=f32)


def iota(shape, dim):
    return lax.broadcasted_iota(jnp.int32, shape, dim)


def ring_index(base, step, size):
    return lax.rem(base + step + size, size)


def head_blocks(n):
    return (iota((n, n), 0) // WIDTH) == (iota((n, n), 1) // WIDTH)


def packed(mapping, state):
    return jnp.concatenate(
        [mapping[:WIDTH] + mapping[WIDTH:], state[:WIDTH] + state[WIDTH:]], axis=0
    ).astype(bf16)


def unpacked(block):
    block = block.astype(f32)
    same = head_blocks(2 * WIDTH)
    mapping, state = block[:WIDTH], block[WIDTH:]
    mapping = jnp.where(same, jnp.concatenate([mapping, mapping], axis=0), 0.0)
    state = jnp.where(same, jnp.concatenate([state, state], axis=0), 0.0)
    return mapping, state


def compose(earlier, latter):
    both = exact(latter[0], jnp.concatenate(earlier, axis=1))
    n = 2 * WIDTH
    return both[:, :n], both[:, n:] + latter[1]


def folded(slots, count, position):
    n = 2 * WIDTH
    eye = jnp.where(iota((n, n), 0) == iota((n, n), 1), 1.0, 0.0)
    before = (eye, jnp.zeros((n, n), f32))
    total = unpacked(slots[0])
    for k in range(1, count):
        hit = position == k
        before = tuple(jnp.where(hit, new, old) for new, old in zip(total, before))
        total = compose(total, unpacked(slots[k]))
    return before, total


def block_inverse(strict):
    n = strict.shape[0]
    row, col = iota((n, n), 0), iota((n, n), 1)
    found = jnp.where(row == col, 1.0, 0.0) + jnp.where(row // 2 == col // 2, strict, 0.0)
    m = 2
    while m < n:
        edge = jnp.where((row // (2 * m) == col // (2 * m)) & (row // m != col // m), strict, 0.0)
        found = found + exact(found, exact(edge, found))
        m *= 2
    return found


def local_mixer(r_ref, k_ref, v_ref, fade_ref, rate_ref):
    r, k, v = r_ref[...].astype(f32), k_ref[...].astype(f32), v_ref[...].astype(f32)
    n = r.shape[0]
    row, col = iota((n, n), 0), iota((n, n), 1)
    ones = jnp.where(head_blocks(n), 1.0, 0.0)
    log_fade = -jax.nn.sigmoid(fade_ref[...]) * 0.6065306597126334
    total_log = exact(jnp.where(row >= col, 1.0, 0.0), log_fade)
    length = jnp.sqrt(exact(k * k, ones))
    unit = k / jnp.maximum(length, 1.0)
    amount = unit * jax.nn.sigmoid(rate_ref[...])
    kept = jnp.exp(total_log)
    grown = jnp.exp(-total_log)
    erase = -unit * jnp.exp(total_log - log_fade)
    read = r * kept
    amount_grown, key_grown = amount * grown, k * grown
    last = kept[n - 1 :, :]
    right = jnp.concatenate([amount_grown, key_grown], axis=0)
    strict, lower = row > col, row >= col
    maps = jnp.zeros((n, n), f32)
    values = jnp.zeros((n, n), f32)
    probe, local_out = read, jnp.zeros((n, n), f32)
    for h in range(n // WIDTH):
        mine = col // WIDTH == h
        erase_h = jnp.where(mine, erase, 0.0)
        read_h = jnp.where(mine, read, 0.0)
        value_h = jnp.where(mine, v, 0.0)
        grams = exact(jnp.concatenate([erase_h, read_h], axis=0), right, NT)
        inverse = block_inverse(jnp.where(strict, grams[:n, :n], 0.0))
        pushed = exact(jnp.where(strict, grams[:n, n:], 0.0), value_h)
        solved = exact(inverse, jnp.concatenate([erase_h, pushed], axis=1))
        shown = exact(jnp.where(lower, grams[n:, :n], 0.0), solved)
        local_out = local_out + shown[:, n:]
        local_out = local_out + exact(jnp.where(lower, grams[n:, n:], 0.0), value_h)
        probe = probe + shown[:, :n]
        maps = maps + solved[:, :n]
        values = values + solved[:, n:]
    same = head_blocks(n)
    amount_end, key_end = amount_grown * last, key_grown * last
    mapping = jnp.where(row == col, last, 0.0) + jnp.where(same, exact(amount_end, maps, TN), 0.0)
    state = jnp.where(same, exact(amount_end, values, TN) + exact(key_end, v, TN), 0.0)
    return mapping, state, probe, local_out


def mixer_kernel(
    nz, ny, span, r_ref, k_ref, v_ref, fade_ref, rate_ref, switch_ref, bonus_ref, rescale_ref,
    gate_ref, up_ref, down_ref, mixed_ref, full_ref,
    near, mid, far, pieces, parts, probe_ref, local_ref, before_ref, carry_ref,
    near_send, near_recv, mid_send, mid_recv, far_send, far_recv, part_send, part_recv,
    plus_send, plus_recv, minus_send, minus_recv,
):
    z, y = lax.axis_index("sp_0"), lax.axis_index("sp_1")
    groups = nz // span
    inner, outer = lax.rem(z, span), z // span
    n = 2 * WIDTH
    units = full_ref.shape[1]
    rows = gate_ref.shape[0]

    def along_y(j):
        return {"sp_1": ring_index(y, j, ny)}

    def along_z(to):
        return {"sp_0": to}

    barrier = pltpu.get_barrier_semaphore()
    for j in range(1, ny):
        pl.semaphore_signal(barrier, inc=1, device_id=along_y(j), device_id_type=MESH)
    for j in range(1, nz):
        pl.semaphore_signal(
            barrier, inc=1, device_id=along_z(ring_index(z, j, nz)), device_id_type=MESH
        )

    mapping, state, probe, local_out = local_mixer(r_ref, k_ref, v_ref, fade_ref, rate_ref)
    near[y] = packed(mapping, state)
    probe_ref[...] = probe
    local_ref[...] = local_out

    eye = jnp.where(iota((rows, rows), 0) == iota((rows, rows), 1), 1.0, 0.0).astype(bf16)
    down_turned = plain(eye, down_ref[...], NT).astype(bf16)
    stacked = jnp.concatenate([gate_ref[...], up_ref[...], down_turned], axis=0)
    wide = pieces.shape[2]
    tall = stacked.shape[1]
    for part in range(ny):
        at, to = iota((tall, wide), 0), iota((tall, wide), 1)
        pick = jnp.where((at == to + part * units) & (to < units), 1.0, 0.0).astype(bf16)
        pieces[part] = plain(stacked, pick).astype(bf16)

    pl.semaphore_wait(barrier, ny - 1 + nz - 1)

    def near_copy(source, target):
        return pltpu.make_async_remote_copy(
            src_ref=near.at[source], dst_ref=near.at[source],
            send_sem=near_send.at[target], recv_sem=near_recv.at[target],
            device_id=along_y(target), device_id_type=MESH,
        )

    def part_copy(j, arriving):
        to = ring_index(y, j, ny)
        source = ring_index(y, -j, ny) if arriving else y
        return pltpu.make_async_remote_copy(
            src_ref=pieces.at[to], dst_ref=parts.at[source],
            send_sem=part_send.at[j], recv_sem=part_recv.at[j],
            device_id=along_y(j), device_id_type=MESH,
        )

    for j in range(1, ny):
        near_copy(y, j).start()
    for j in range(1, ny):
        part_copy(j, False).start()
    parts[y] = pieces[y]

    for j in range(1, ny):
        near_copy(ring_index(y, -j, ny), j).wait_recv()
    before, total = folded(near, ny, y)
    before_ref[0] = before[0]
    before_ref[1] = before[1]

    def mid_copy(source, j):
        to = z - inner + ring_index(inner, j, span)
        return pltpu.make_async_remote_copy(
            src_ref=mid.at[source], dst_ref=mid.at[source],
            send_sem=mid_send.at[j], recv_sem=mid_recv.at[j],
            device_id=along_z(to), device_id_type=MESH,
        )

    mid[inner] = packed(*total)
    for j in range(1, span):
        mid_copy(inner, j).start()

    for j in range(1, ny):
        part_copy(j, True).wait_recv()
    square = jnp.where(iota((units, wide), 0) == iota((units, wide), 1), 1.0, 0.0).astype(bf16)
    for c in range(3):
        tallest = jnp.concatenate(
            [parts[part, c * rows : (c + 1) * rows, :] for part in range(ny)], axis=0
        )
        block = plain(square, tallest, NT).astype(bf16)
        full_ref[c, :, pl.ds(pl.multiple_of(z * ny * rows, ny * rows), ny * rows)] = block

    def piece(c, at):
        return full_ref.at[c, :, pl.ds(pl.multiple_of(at * ny * rows, ny * rows), ny * rows)]

    def plus_copy(c, s, at):
        return pltpu.make_async_remote_copy(
            src_ref=piece(c, at), dst_ref=piece(c, at),
            send_sem=plus_send.at[c, s], recv_sem=plus_recv.at[c, s],
            device_id=along_z(ring_index(z, 1, nz)), device_id_type=MESH,
        )

    def minus_copy(c, s, at):
        return pltpu.make_async_remote_copy(
            src_ref=piece(c, at), dst_ref=piece(c, at),
            send_sem=minus_send.at[c, s], recv_sem=minus_recv.at[c, s],
            device_id=along_z(ring_index(z, -1, nz)), device_id_type=MESH,
        )

    n_plus = nz // 2
    n_minus = nz - 1 - n_plus

    def ring_step(s):
        for c in range(3):
            if s > 0 and s <= n_plus:
                plus_copy(c, s - 1, ring_index(z, -s, nz)).wait_recv()
            if s < n_plus:
                plus_copy(c, s, ring_index(z, -s, nz)).start()
            if s > 0 and s <= n_minus:
                minus_copy(c, s - 1, ring_index(z, s, nz)).wait_recv()
            if s < n_minus:
                minus_copy(c, s, ring_index(z, s, nz)).start()

    ring_step(0)

    for j in range(1, span):
        mid_copy(ring_index(inner, -j, span), j).wait_recv()
    before_z, total_z = folded(mid, span, inner)
    before_ref[2] = before_z[0]
    before_ref[3] = before_z[1]

    def far_copy(slot, d, to):
        return pltpu.make_async_remote_copy(
            src_ref=far.at[slot], dst_ref=far.at[slot],
            send_sem=far_send.at[d], recv_sem=far_recv.at[d],
            device_id=along_z(to), device_id_type=MESH,
        )

    far[outer] = packed(*total_z)
    for d in range(1, groups):
        @pl.when(outer + d < groups)
        def _():
            far_copy(outer, d, lax.rem(z + d * span, nz)).start()

    steps = n_plus + 1
    early = min(2, steps - 1)
    for s in range(1, 1 + early):
        ring_step(s)

    carry_ref[...] = jnp.zeros((n, n), f32)
    for g in range(groups - 1):
        @pl.when(outer > g)
        def _():
            for d in range(1, groups):
                @pl.when(outer - g == d)
                def _():
                    far_copy(g, d, lax.rem(z + d * span, nz)).wait_recv()
            step = unpacked(far[g])
            carry_ref[...] = exact(step[0], carry_ref[...]) + step[1]
    incoming = exact(before_ref[2], carry_ref[...]) + before_ref[3]
    incoming = exact(before_ref[0], incoming) + before_ref[1]

    closing = local_ref[...] + exact(probe_ref[...], incoming)
    ones = jnp.where(head_blocks(n), 1.0, 0.0)
    centred = closing - exact(closing, ones) * (1.0 / WIDTH)
    spread = exact(centred * centred, ones) * (1.0 / WIDTH)
    rescaled = centred * lax.rsqrt(spread + group_eps) * rescale_ref[...]
    value = v_ref[...].astype(f32)
    bonus = exact(r_ref[...].astype(f32) * k_ref[...].astype(f32) * bonus_ref[...], ones) * value
    mixed_ref[...] = ((rescaled + bonus) * switch_ref[...].astype(f32)).astype(bf16)

    for s in range(1 + early, steps):
        ring_step(s)

    for j in range(1, ny):
        near_copy(y, j).wait_send()
        part_copy(j, False).wait_send()
    for j in range(1, span):
        mid_copy(inner, j).wait_send()
    for d in range(1, groups):
        @pl.when(outer + d < groups)
        def _():
            far_copy(outer, d, lax.rem(z + d * span, nz)).wait_send()
    for c in range(3):
        for s in range(n_plus):
            plus_copy(c, s, ring_index(z, -s, nz)).wait_send()
        for s in range(n_minus):
            minus_copy(c, s, ring_index(z, s, nz)).wait_send()


def mixer_and_weights(r, k, v, fade, rate, switch, bonus, rescale, gate, up, down):
    nz, ny = lax.axis_size("sp_0"), lax.axis_size("sp_1")
    span = min(4, nz)
    groups = nz // span
    n = r.shape[0]
    rows, hidden = gate.shape
    units = hidden // ny
    wide = -(-units // 128) * 128
    dma = pltpu.SemaphoreType.DMA
    block = pltpu.VMEM((n, n), bf16)
    in_vmem = pl.BlockSpec(memory_space=pltpu.VMEM)
    n_plus = nz // 2
    return pl.pallas_call(
        functools.partial(mixer_kernel, nz, ny, span),
        out_shape=(
            jax.ShapeDtypeStruct((n, n), bf16),
            jax.ShapeDtypeStruct((3, units, nz * ny * rows), bf16),
        ),
        in_specs=[in_vmem] * 11,
        out_specs=(in_vmem, in_vmem),
        scratch_shapes=[
            pltpu.VMEM((ny, n, n), bf16),
            pltpu.VMEM((span, n, n), bf16),
            pltpu.VMEM((groups, n, n), bf16),
            pltpu.VMEM((ny, 3 * rows, wide), bf16),
            pltpu.VMEM((ny, 3 * rows, wide), bf16),
            pltpu.VMEM((n, n), f32),
            pltpu.VMEM((n, n), f32),
            pltpu.VMEM((4, n, n), f32),
            pltpu.VMEM((n, n), f32),
            dma((ny,)), dma((ny,)), dma((span,)), dma((span,)), dma((groups,)), dma((groups,)),
            dma((ny,)), dma((ny,)),
            dma((3, n_plus)), dma((3, n_plus)), dma((3, n_plus)), dma((3, n_plus)),
        ],
        compiler_params=pltpu.CompilerParams(collective_id=0, has_side_effects=True),
        cost_estimate=pl.CostEstimate(flops=2 * 10**9, bytes_accessed=4 * 10**6, transcendentals=0),
        name="mixer",
    )(r, k, v, fade, rate, switch, bonus, rescale, gate, up, down)


def in_blocks(shard, count):
    return shard.reshape(count, -1, shard.shape[1])


def summed_on_arrival(shard, axis):
    count = lax.axis_size(axis)
    tiles = lax.all_to_all(in_blocks(shard, count), axis, 0, 0, tiled=True)
    return jnp.sum(tiles.astype(f32), axis=0)


def body(
    r, k, v, fade, rate, switch, bonus, rescale, exit_weights, skip, scaling, gate, up, taps, down
):
    nz = lax.axis_size("sp_0")
    mixed, weights = mixer_and_weights(
        r, k, v, fade, rate, switch, bonus[None], rescale[None], gate, up, down
    )
    attended = summed_on_arrival(
        jnp.dot(mixed, exit_weights, preferred_element_type=f32).astype(bf16), "tp"
    )
    hidden_res = skip.astype(f32) + attended
    normed = (
        hidden_res
        * lax.rsqrt(jnp.mean(hidden_res * hidden_res, axis=-1, keepdims=True) + norm_eps)
        * scaling
    ).astype(bf16)
    rows = lax.all_gather(normed, ("sp_1", "tp"), tiled=True)
    gate_pre = plain(rows, weights[0], NT).astype(bf16)
    up_part = plain(rows, weights[1], NT).astype(bf16)
    count = taps.shape[0]
    units = gate_pre.shape[1]
    route = [(i, i + 1) for i in range(nz - 1)]
    tail = lax.ppermute(gate_pre[gate_pre.shape[0] - count + 1 :], "sp_0", route)
    mine = lax.dynamic_slice_in_dim(taps, lax.axis_index("sp_1") * units, units, axis=1)
    extended = jnp.concatenate([tail, gate_pre], axis=0).astype(f32)
    conv = jnp.zeros(gate_pre.shape, f32)
    for tap in range(count):
        conv = conv + mine[tap] * extended[tap : tap + gate_pre.shape[0]]
    hidden = (jax.nn.silu(conv) * up_part.astype(f32)).astype(bf16)
    projected = summed_on_arrival(plain(hidden, weights[2]).astype(bf16), ("sp_1", "tp"))
    return (hidden_res + projected).astype(bf16)


def solution(mesh):
    sp, tp = mesh.shape["sp"], mesh.shape["tp"]
    ny = COLUMNS
    finer = Mesh(mesh.devices.reshape(sp // ny, ny, tp), SP_TP)
    cut = P(SP, "tp")
    placed = (
        cut, cut, cut, cut, cut, cut, P("tp"), P("tp"), P("tp", None), P(SP_TP, None), P(),
        cut, cut, P(None, "tp"), P("tp", SP),
    )
    return jax.shard_map(
        body, mesh=finer, in_specs=placed, out_specs=P(SP_TP, None), check_vma=False
    )
```

```python
import functools

import jax
import jax.numpy as jnp
from jax import lax
from jax.experimental import pallas as pl
from jax.experimental.pallas import tpu as pltpu
from jax.sharding import Mesh
from jax.sharding import PartitionSpec as P

WIDTH = 64
SP = ("sp_0", "sp_1")
SP_TP = ("sp_0", "sp_1", "tp")
COLUMNS = 4
MESH = pl.DeviceIdType.MESH

group_eps = 0.00064
norm_eps = 1e-06
f32 = jnp.float32
bf16 = jnp.bfloat16

NN = (((1,), (0,)), ((), ()))
NT = (((1,), (1,)), ((), ()))
TN = (((0,), (0,)), ((), ()))


def exact(a, b, dims=NN):
    return lax.dot_general(
        a, b, dims, precision=lax.Precision.HIGHEST, preferred_element_type=f32
    )


def plain(a, b, dims=NN):
    return lax.dot_general(a, b, dims, preferred_element_type=f32)


def iota(shape, dim):
    return lax.broadcasted_iota(jnp.int32, shape, dim)


def ring_index(base, step, size):
    return lax.rem(base + step + size, size)


def head_blocks(n):
    return (iota((n, n), 0) // WIDTH) == (iota((n, n), 1) // WIDTH)


def packed(mapping, state):
    return jnp.concatenate(
        [mapping[:WIDTH] + mapping[WIDTH:], state[:WIDTH] + state[WIDTH:]], axis=0
    ).astype(bf16)


def unpacked(block):
    block = block.astype(f32)
    same = head_blocks(2 * WIDTH)
    mapping, state = block[:WIDTH], block[WIDTH:]
    mapping = jnp.where(same, jnp.concatenate([mapping, mapping], axis=0), 0.0)
    state = jnp.where(same, jnp.concatenate([state, state], axis=0), 0.0)
    return mapping, state


def compose(earlier, latter):
    both = exact(latter[0], jnp.concatenate(earlier, axis=1))
    n = 2 * WIDTH
    return both[:, :n], both[:, n:] + latter[1]


def folded(slots, count, position):
    n = 2 * WIDTH
    eye = jnp.where(iota((n, n), 0) == iota((n, n), 1), 1.0, 0.0)
    before = (eye, jnp.zeros((n, n), f32))
    total = unpacked(slots[0])
    for k in range(1, count):
        hit = position == k
        before = tuple(jnp.where(hit, new, old) for new, old in zip(total, before))
        total = compose(total, unpacked(slots[k]))
    return before, total


def block_inverse(strict):
    n = strict.shape[0]
    row, col = iota((n, n), 0), iota((n, n), 1)
    found = jnp.where(row == col, 1.0, 0.0) + jnp.where(row // 2 == col // 2, strict, 0.0)
    m = 2
    while m < n:
        edge = jnp.where((row // (2 * m) == col // (2 * m)) & (row // m != col // m), strict, 0.0)
        found = found + exact(found, exact(edge, found))
        m *= 2
    return found


def local_mixer(r_ref, k_ref, v_ref, fade_ref, rate_ref):
    r, k, v = r_ref[...].astype(f32), k_ref[...].astype(f32), v_ref[...].astype(f32)
    n = r.shape[0]
    row, col = iota((n, n), 0), iota((n, n), 1)
    ones = jnp.where(head_blocks(n), 1.0, 0.0)
    log_fade = -jax.nn.sigmoid(fade_ref[...]) * 0.6065306597126334
    total_log = exact(jnp.where(row >= col, 1.0, 0.0), log_fade)
    length = jnp.sqrt(exact(k * k, ones))
    unit = k / jnp.maximum(length, 1.0)
    amount = unit * jax.nn.sigmoid(rate_ref[...])
    kept = jnp.exp(total_log)
    grown = jnp.exp(-total_log)
    erase = -unit * jnp.exp(total_log - log_fade)
    read = r * kept
    amount_grown, key_grown = amount * grown, k * grown
    last = kept[n - 1 :, :]
    right = jnp.concatenate([amount_grown, key_grown], axis=0)
    strict, lower = row > col, row >= col
    maps = jnp.zeros((n, n), f32)
    values = jnp.zeros((n, n), f32)
    probe, local_out = read, jnp.zeros((n, n), f32)
    for h in range(n // WIDTH):
        mine = col // WIDTH == h
        erase_h = jnp.where(mine, erase, 0.0)
        read_h = jnp.where(mine, read, 0.0)
        value_h = jnp.where(mine, v, 0.0)
        grams = exact(jnp.concatenate([erase_h, read_h], axis=0), right, NT)
        inverse = block_inverse(jnp.where(strict, grams[:n, :n], 0.0))
        pushed = exact(jnp.where(strict, grams[:n, n:], 0.0), value_h)
        solved = exact(inverse, jnp.concatenate([erase_h, pushed], axis=1))
        shown = exact(jnp.where(lower, grams[n:, :n], 0.0), solved)
        local_out = local_out + shown[:, n:]
        local_out = local_out + exact(jnp.where(lower, grams[n:, n:], 0.0), value_h)
        probe = probe + shown[:, :n]
        maps = maps + solved[:, :n]
        values = values + solved[:, n:]
    same = head_blocks(n)
    amount_end, key_end = amount_grown * last, key_grown * last
    mapping = jnp.where(row == col, last, 0.0) + jnp.where(same, exact(amount_end, maps, TN), 0.0)
    state = jnp.where(same, exact(amount_end, values, TN) + exact(key_end, v, TN), 0.0)
    return mapping, state, probe, local_out


def layer_kernel(
    nz, ny, nt, span, r_ref, k_ref, v_ref, fade_ref, rate_ref, switch_ref, bonus_ref, rescale_ref,
    exit_ref, skip_ref, scaling_ref, gate_ref, up_ref, taps_ref, down_ref, out_ref,
    full_ref, near, mid, far, pieces, parts, probe_ref, local_ref, before_ref, carry_ref,
    sent, landed, stream_ref, rows_ref, gate_scr, edge_out, edge_in, partial, swapped, summed,
    first, second, final,
    near_send, near_recv, mid_send, mid_recv, far_send, far_recv, part_send, part_recv,
    plus_send, plus_recv, minus_send, minus_recv,
    exit_send, exit_recv, one_send, one_recv, two_send, two_recv, pair_send, pair_recv,
    edge_send, edge_recv, swap_send, swap_recv, first_send, first_recv, last_send, last_recv,
):
    z, y, t = lax.axis_index("sp_0"), lax.axis_index("sp_1"), lax.axis_index("tp")
    nx = nt // 2
    x, core = t // 2, lax.rem(t, 2)
    groups = nz // span
    inner, outer = lax.rem(z, span), z // span
    n = 2 * WIDTH
    units = full_ref.shape[1]
    rows = gate_ref.shape[0]

    def along_y(j):
        return {"sp_1": ring_index(y, j, ny)}

    def along_z(to):
        return {"sp_0": to}

    barrier = pltpu.get_barrier_semaphore()
    for j in range(1, ny):
        pl.semaphore_signal(barrier, inc=1, device_id=along_y(j), device_id_type=MESH)
    for j in range(1, nz):
        pl.semaphore_signal(
            barrier, inc=1, device_id=along_z(ring_index(z, j, nz)), device_id_type=MESH
        )
    for j in range(1, nt):
        pl.semaphore_signal(
            barrier, inc=1, device_id={"tp": ring_index(t, j, nt)}, device_id_type=MESH
        )

    mapping, state, probe, local_out = local_mixer(r_ref, k_ref, v_ref, fade_ref, rate_ref)
    near[y] = packed(mapping, state)
    probe_ref[...] = probe
    local_ref[...] = local_out

    eye = jnp.where(iota((rows, rows), 0) == iota((rows, rows), 1), 1.0, 0.0).astype(bf16)
    down_turned = plain(eye, down_ref[...], NT).astype(bf16)
    stacked = jnp.concatenate([gate_ref[...], up_ref[...], down_turned], axis=0)
    wide = pieces.shape[2]
    tall = stacked.shape[1]
    for part in range(ny):
        at, to = iota((tall, wide), 0), iota((tall, wide), 1)
        pick = jnp.where((at == to + part * units) & (to < units), 1.0, 0.0).astype(bf16)
        pieces[part] = plain(stacked, pick).astype(bf16)

    pl.semaphore_wait(barrier, ny - 1 + nz - 1 + nt - 1)

    def near_copy(source, target):
        return pltpu.make_async_remote_copy(
            src_ref=near.at[source], dst_ref=near.at[source],
            send_sem=near_send.at[target], recv_sem=near_recv.at[target],
            device_id=along_y(target), device_id_type=MESH,
        )

    def part_copy(j, arriving):
        to = ring_index(y, j, ny)
        source = ring_index(y, -j, ny) if arriving else y
        return pltpu.make_async_remote_copy(
            src_ref=pieces.at[to], dst_ref=parts.at[source],
            send_sem=part_send.at[j], recv_sem=part_recv.at[j],
            device_id=along_y(j), device_id_type=MESH,
        )

    for j in range(1, ny):
        near_copy(y, j).start()
    for j in range(1, ny):
        part_copy(j, False).start()
    parts[y] = pieces[y]

    for j in range(1, ny):
        near_copy(ring_index(y, -j, ny), j).wait_recv()
    before, total = folded(near, ny, y)
    before_ref[0] = before[0]
    before_ref[1] = before[1]

    def mid_copy(source, j):
        to = z - inner + ring_index(inner, j, span)
        return pltpu.make_async_remote_copy(
            src_ref=mid.at[source], dst_ref=mid.at[source],
            send_sem=mid_send.at[j], recv_sem=mid_recv.at[j],
            device_id=along_z(to), device_id_type=MESH,
        )

    mid[inner] = packed(*total)
    for j in range(1, span):
        mid_copy(inner, j).start()

    for j in range(1, ny):
        part_copy(j, True).wait_recv()
    square = jnp.where(iota((units, wide), 0) == iota((units, wide), 1), 1.0, 0.0).astype(bf16)
    for c in range(3):
        tallest = jnp.concatenate(
            [parts[part, c * rows : (c + 1) * rows, :] for part in range(ny)], axis=0
        )
        block = plain(square, tallest, NT).astype(bf16)
        full_ref[c, :, pl.ds(pl.multiple_of(z * ny * rows, ny * rows), ny * rows)] = block

    def piece(c, at):
        return full_ref.at[c, :, pl.ds(pl.multiple_of(at * ny * rows, ny * rows), ny * rows)]

    def plus_copy(c, s, at):
        return pltpu.make_async_remote_copy(
            src_ref=piece(c, at), dst_ref=piece(c, at),
            send_sem=plus_send.at[c, s], recv_sem=plus_recv.at[c, s],
            device_id=along_z(ring_index(z, 1, nz)), device_id_type=MESH,
        )

    def minus_copy(c, s, at):
        return pltpu.make_async_remote_copy(
            src_ref=piece(c, at), dst_ref=piece(c, at),
            send_sem=minus_send.at[c, s], recv_sem=minus_recv.at[c, s],
            device_id=along_z(ring_index(z, -1, nz)), device_id_type=MESH,
        )

    n_plus = nz // 2
    n_minus = nz - 1 - n_plus

    def ring_step(s):
        for c in range(3):
            if s > 0 and s <= n_plus:
                plus_copy(c, s - 1, ring_index(z, -s, nz)).wait_recv()
            if s < n_plus:
                plus_copy(c, s, ring_index(z, -s, nz)).start()
            if s > 0 and s <= n_minus:
                minus_copy(c, s - 1, ring_index(z, s, nz)).wait_recv()
            if s < n_minus:
                minus_copy(c, s, ring_index(z, s, nz)).start()

    ring_step(0)

    for j in range(1, span):
        mid_copy(ring_index(inner, -j, span), j).wait_recv()
    before_z, total_z = folded(mid, span, inner)
    before_ref[2] = before_z[0]
    before_ref[3] = before_z[1]

    def far_copy(slot, d, to):
        return pltpu.make_async_remote_copy(
            src_ref=far.at[slot], dst_ref=far.at[slot],
            send_sem=far_send.at[d], recv_sem=far_recv.at[d],
            device_id=along_z(to), device_id_type=MESH,
        )

    far[outer] = packed(*total_z)
    for d in range(1, groups):
        @pl.when(outer + d < groups)
        def _():
            far_copy(outer, d, lax.rem(z + d * span, nz)).start()

    steps = n_plus + 1
    early = min(3, steps - 1)
    for s in range(1, 1 + early):
        ring_step(s)

    carry_ref[...] = jnp.zeros((n, n), f32)
    for g in range(groups - 1):
        @pl.when(outer > g)
        def _():
            for d in range(1, groups):
                @pl.when(outer - g == d)
                def _():
                    far_copy(g, d, lax.rem(z + d * span, nz)).wait_recv()
            step = unpacked(far[g])
            carry_ref[...] = exact(step[0], carry_ref[...]) + step[1]
    incoming = exact(before_ref[2], carry_ref[...]) + before_ref[3]
    incoming = exact(before_ref[0], incoming) + before_ref[1]

    closing = local_ref[...] + exact(probe_ref[...], incoming)
    ones = jnp.where(head_blocks(n), 1.0, 0.0)
    centred = closing - exact(closing, ones) * (1.0 / WIDTH)
    spread = exact(centred * centred, ones) * (1.0 / WIDTH)
    rescaled = centred * lax.rsqrt(spread + group_eps) * rescale_ref[...]
    value = v_ref[...].astype(f32)
    bonus = exact(r_ref[...].astype(f32) * k_ref[...].astype(f32) * bonus_ref[...], ones) * value
    mixed = ((rescaled + bonus) * switch_ref[...].astype(f32)).astype(bf16)

    pending = list(range(1 + early, steps))

    def ring_steps(count):
        for s in pending[:count]:
            ring_step(s)
        del pending[:count]

    own = n // nt
    width = exit_ref.shape[1]

    def exit_copy(j):
        to = ring_index(t, j, nt)
        return pltpu.make_async_remote_copy(
            src_ref=sent.at[to], dst_ref=landed.at[j],
            send_sem=exit_send.at[j], recv_sem=exit_recv.at[j],
            device_id={"tp": to}, device_id_type=MESH,
        )

    sent[...] = plain(mixed, exit_ref[...]).astype(bf16).reshape(nt, own, width)
    for j in range(1, nt):
        exit_copy(j).start()
    ring_steps(2)
    attended = sent[t].astype(f32)
    for j in range(1, nt):
        exit_copy(j).wait_recv()
    for j in range(1, nt):
        attended = attended + landed[j].astype(f32)
    stream = skip_ref[...].astype(f32) + attended
    stream_ref[...] = stream
    mean = jnp.mean(stream * stream, axis=-1, keepdims=True)
    rows_ref[y, x, core] = (stream * lax.rsqrt(mean + norm_eps) * scaling_ref[...]).astype(bf16)

    across = 1 - core
    na = ny
    a, b = y * across + x * core, x * across + y * core

    def place(a_to, b_to):
        return a_to * across + b_to * core, b_to * across + a_to * core

    def device(a_to, b_to):
        y_to, x_to = place(a_to, b_to)
        return {"sp_1": y_to, "tp": 2 * x_to + core}

    def slot(j, i):
        y_at, x_at = place(ring_index(a, -j, na), ring_index(b, -i, na))
        return rows_ref.at[y_at, x_at, core]

    def one_copy(j, arriving):
        ref = slot(0, j if arriving else 0)
        return pltpu.make_async_remote_copy(
            src_ref=ref, dst_ref=ref, send_sem=one_send.at[j], recv_sem=one_recv.at[j],
            device_id=device(a, ring_index(b, j, na)), device_id_type=MESH,
        )

    def two_copy(j, i, arriving):
        ref = slot(j if arriving else 0, i)
        return pltpu.make_async_remote_copy(
            src_ref=ref, dst_ref=ref, send_sem=two_send.at[j, i], recv_sem=two_recv.at[j, i],
            device_id=device(ring_index(a, j, na), b), device_id_type=MESH,
        )

    partner = {"tp": t + 1 - 2 * core}

    def pair_copy(j, i, arriving):
        if arriving:
            y_at, x_at = place(ring_index(a, -i, na), ring_index(b, -j, na))
            ref = rows_ref.at[y_at, x_at, 1 - core]
        else:
            ref = slot(j, i)
        return pltpu.make_async_remote_copy(
            src_ref=ref, dst_ref=ref, send_sem=pair_send.at[j, i], recv_sem=pair_recv.at[j, i],
            device_id=partner, device_id_type=MESH,
        )

    for j in range(1, na):
        one_copy(j, False).start()
    for j in range(1, na):
        two_copy(j, 0, False).start()
    pair_copy(0, 0, False).start()
    for i in range(1, na):
        one_copy(i, True).wait_recv()
        for j in range(1, na):
            two_copy(j, i, False).start()
        pair_copy(0, i, False).start()
    ring_steps(len(pending))
    units_at = iota((taps_ref.shape[1], units), 0) == iota((taps_ref.shape[1], units), 1) + y * units
    taps = exact(taps_ref[...], jnp.where(units_at, 1.0, 0.0))
    for i in range(na):
        for j in range(1, na):
            two_copy(j, i, True).wait_recv()
            pair_copy(j, i, False).start()
    for i in range(na):
        for j in range(na):
            pair_copy(j, i, True).wait_recv()

    tokens = na * n
    rows_all = rows_ref[...].reshape(tokens, width)
    gate_pre = plain(rows_all, full_ref[0], NT).astype(bf16)
    edge = edge_out.shape[0]
    edge_out[...] = gate_pre[tokens - edge :, :]

    def edge_copy():
        return pltpu.make_async_remote_copy(
            src_ref=edge_out, dst_ref=edge_in, send_sem=edge_send.at[0], recv_sem=edge_recv.at[0],
            device_id=along_z(ring_index(z, 1, nz)), device_id_type=MESH,
        )

    @pl.when(z < nz - 1)
    def _():
        edge_copy().start()

    gate_scr[edge:, :] = gate_pre.astype(f32)
    up_part = plain(rows_all, full_ref[1], NT).astype(bf16)

    @pl.when(z > 0)
    def _():
        edge_copy().wait_recv()
        gate_scr[:edge, :] = edge_in[...].astype(f32)

    @pl.when(z == 0)
    def _():
        gate_scr[:edge, :] = jnp.zeros((edge, units), f32)

    count = taps_ref.shape[0]
    conv = jnp.zeros((tokens, units), f32)
    for tap in range(count):
        start = edge - count + 1 + tap
        conv = conv + taps[tap : tap + 1, :] * gate_scr[start : start + tokens, :]
    hidden = (conv / (1.0 + jnp.exp(-conv)) * up_part.astype(f32)).astype(bf16)

    def swap_copy(part):
        return pltpu.make_async_remote_copy(
            src_ref=partial.at[part, :, 1 - core], dst_ref=swapped.at[part],
            send_sem=swap_send.at[part], recv_sem=swap_recv.at[part],
            device_id=partner, device_id_type=MESH,
        )

    for part in range(ny):
        product = plain(hidden[part * n : (part + 1) * n, :], full_ref[2]).astype(bf16)
        partial[part] = product.reshape(nx, 2, own, width)
        swap_copy(part).start()

    def first_copy(j):
        return pltpu.make_async_remote_copy(
            src_ref=summed.at[ring_index(a, j, na)], dst_ref=first.at[j],
            send_sem=first_send.at[j], recv_sem=first_recv.at[j],
            device_id=device(ring_index(a, j, na), b), device_id_type=MESH,
        )

    for part in range(ny):
        swap_copy(part).wait_recv()
    for j in list(range(1, na)) + [0]:
        a_to = ring_index(a, j, na)
        for b_to in range(na):
            y_at, x_at = place(a_to, b_to)
            both = partial[y_at, x_at, core].astype(f32) + swapped[y_at, x_at].astype(f32)
            summed[a_to, b_to] = both.astype(bf16)
        if j > 0:
            first_copy(j).start()

    def last_copy(j):
        return pltpu.make_async_remote_copy(
            src_ref=second.at[ring_index(b, j, na)], dst_ref=final.at[j],
            send_sem=last_send.at[j], recv_sem=last_recv.at[j],
            device_id=device(a, ring_index(b, j, na)), device_id_type=MESH,
        )

    for j in range(1, na):
        first_copy(j).wait_recv()
    for j in list(range(1, na)) + [0]:
        b_to = ring_index(b, j, na)
        total_rows = summed[a, b_to].astype(f32)
        for i in range(1, na):
            total_rows = total_rows + first[i, b_to].astype(f32)
        second[b_to] = total_rows.astype(bf16)
        if j > 0:
            last_copy(j).start()
    projected = second[b].astype(f32)
    for j in range(1, na):
        last_copy(j).wait_recv()
    for j in range(1, na):
        projected = projected + final[j].astype(f32)
    out_ref[...] = (stream_ref[...] + projected).astype(bf16)

    for j in range(1, ny):
        near_copy(y, j).wait_send()
        part_copy(j, False).wait_send()
    for j in range(1, span):
        mid_copy(inner, j).wait_send()
    for d in range(1, groups):
        @pl.when(outer + d < groups)
        def _():
            far_copy(outer, d, lax.rem(z + d * span, nz)).wait_send()
    for c in range(3):
        for s in range(n_plus):
            plus_copy(c, s, ring_index(z, -s, nz)).wait_send()
        for s in range(n_minus):
            minus_copy(c, s, ring_index(z, s, nz)).wait_send()
    for j in range(1, nt):
        exit_copy(j).wait_send()
    for j in range(1, na):
        one_copy(j, False).wait_send()
        first_copy(j).wait_send()
        last_copy(j).wait_send()
        for i in range(na):
            two_copy(j, i, False).wait_send()
    for i in range(na):
        for j in range(na):
            pair_copy(j, i, False).wait_send()
    for part in range(ny):
        swap_copy(part).wait_send()

    @pl.when(z < nz - 1)
    def _():
        edge_copy().wait_send()


def layer(r, k, v, fade, rate, switch, bonus, rescale, leave, skip, scaling, gate, up, taps, down):
    nz, ny, nt = lax.axis_size("sp_0"), lax.axis_size("sp_1"), lax.axis_size("tp")
    span = min(4, nz)
    groups = nz // span
    nx = nt // 2
    n = r.shape[0]
    rows, hidden = gate.shape
    units = hidden // ny
    wide = -(-units // 128) * 128
    own, width = skip.shape
    dma = pltpu.SemaphoreType.DMA
    in_vmem = pl.BlockSpec(memory_space=pltpu.VMEM)
    n_plus = nz // 2
    edge = 16
    return pl.pallas_call(
        functools.partial(layer_kernel, nz, ny, nt, span),
        out_shape=jax.ShapeDtypeStruct((own, width), bf16),
        in_specs=[in_vmem] * 15,
        out_specs=in_vmem,
        scratch_shapes=[
            pltpu.VMEM((3, units, nz * ny * rows), bf16),
            pltpu.VMEM((ny, n, n), bf16),
            pltpu.VMEM((span, n, n), bf16),
            pltpu.VMEM((groups, n, n), bf16),
            pltpu.VMEM((ny, 3 * rows, wide), bf16),
            pltpu.VMEM((ny, 3 * rows, wide), bf16),
            pltpu.VMEM((n, n), f32),
            pltpu.VMEM((n, n), f32),
            pltpu.VMEM((4, n, n), f32),
            pltpu.VMEM((n, n), f32),
            pltpu.VMEM((nt, own, width), bf16),
            pltpu.VMEM((nt, own, width), bf16),
            pltpu.VMEM((own, width), f32),
            pltpu.VMEM((ny, nx, 2, own, width), bf16),
            pltpu.VMEM((edge + ny * n, units), f32),
            pltpu.VMEM((edge, units), bf16),
            pltpu.VMEM((edge, units), bf16),
            pltpu.VMEM((ny, nx, 2, own, width), bf16),
            pltpu.VMEM((ny, nx, own, width), bf16),
            pltpu.VMEM((ny, nx, own, width), bf16),
            pltpu.VMEM((ny, nx, own, width), bf16),
            pltpu.VMEM((nx, own, width), bf16),
            pltpu.VMEM((nx, own, width), bf16),
            dma((ny,)), dma((ny,)), dma((span,)), dma((span,)), dma((groups,)), dma((groups,)),
            dma((ny,)), dma((ny,)),
            dma((3, n_plus)), dma((3, n_plus)), dma((3, n_plus)), dma((3, n_plus)),
            dma((nt,)), dma((nt,)), dma((nx,)), dma((nx,)),
            dma((ny, nx)), dma((ny, nx)), dma((ny, nx)), dma((ny, nx)),
            dma((1,)), dma((1,)), dma((ny,)), dma((ny,)),
            dma((ny,)), dma((ny,)), dma((nx,)), dma((nx,)),
        ],
        compiler_params=pltpu.CompilerParams(
            collective_id=0, has_side_effects=True, vmem_limit_bytes=48 * 2**20
        ),
        name="layer",
    )(r, k, v, fade, rate, switch, bonus, rescale, leave, skip, scaling, gate, up, taps, down)


def body(
    r, k, v, fade, rate, switch, bonus, rescale, leave, skip, scaling, gate, up, taps, down
):
    return layer(
        r, k, v, fade, rate, switch, bonus[None], rescale[None], leave, skip, scaling[None],
        gate, up, taps, down,
    )


def solution(mesh):
    sp, tp = mesh.shape["sp"], mesh.shape["tp"]
    ny = COLUMNS
    finer = Mesh(mesh.devices.reshape(sp // ny, ny, tp), SP_TP)
    cut = P(SP, "tp")
    placed = (
        cut, cut, cut, cut, cut, cut, P("tp"), P("tp"), P("tp", None), P(SP_TP, None), P(),
        cut, cut, P(None, "tp"), P("tp", SP),
    )
    return jax.shard_map(
        body, mesh=finer, in_specs=placed, out_specs=P(SP_TP, None), check_vma=False
    )
```

```python
import functools

import jax
import jax.numpy as jnp
from jax import lax
from jax.experimental import pallas as pl
from jax.experimental.pallas import tpu as pltpu
from jax.sharding import Mesh
from jax.sharding import PartitionSpec as P

WIDTH = 64
SP = ("sp_0", "sp_1")
SP_TP = ("sp_0", "sp_1", "tp")
COLUMNS = 4
BANDS = 4
SPLIT = 16
FIRST, SECOND, MIDDLE, LATE = 1, 2, 2, 1
MESH = pl.DeviceIdType.MESH

group_eps = 0.00064
norm_eps = 1e-06
f32 = jnp.float32
bf16 = jnp.bfloat16

NN = (((1,), (0,)), ((), ()))
NT = (((1,), (1,)), ((), ()))
TN = (((0,), (0,)), ((), ()))


def exact(a, b, dims=NN):
    return lax.dot_general(
        a, b, dims, precision=lax.Precision.HIGHEST, preferred_element_type=f32
    )


def plain(a, b, dims=NN):
    return lax.dot_general(a, b, dims, preferred_element_type=f32)


def split(a):
    high = a.astype(bf16)
    return high, (a - high.astype(f32)).astype(bf16)


def fine(a, b, dims=NN):
    (a_dim,), (b_dim,) = dims[0]
    a_high, a_low = split(a)
    b_high, b_low = split(b)
    left = jnp.concatenate([a_high, a_high, a_low], axis=a_dim)
    right = jnp.concatenate([b_high, b_low, b_high], axis=b_dim)
    return plain(left, right, dims)


def left_exact(a, b):
    a = a.astype(bf16)
    return plain(jnp.concatenate([a, a], axis=1), jnp.concatenate(split(b), axis=0))


def right_exact(a, b):
    b = b.astype(bf16)
    return plain(jnp.concatenate(split(a), axis=1), jnp.concatenate([b, b], axis=0))


def iota(shape, dim):
    return lax.broadcasted_iota(jnp.int32, shape, dim)


def ring_index(base, step, size):
    return lax.rem(base + step + size, size)


def head_blocks(n):
    return (iota((n, n), 0) // WIDTH) == (iota((n, n), 1) // WIDTH)


def packed(mapping, state):
    return jnp.concatenate(
        [mapping[:WIDTH] + mapping[WIDTH:], state[:WIDTH] + state[WIDTH:]], axis=0
    ).astype(bf16)


def unpacked(block):
    block = block.astype(f32)
    same = head_blocks(2 * WIDTH)
    mapping, state = block[:WIDTH], block[WIDTH:]
    mapping = jnp.where(same, jnp.concatenate([mapping, mapping], axis=0), 0.0)
    state = jnp.where(same, jnp.concatenate([state, state], axis=0), 0.0)
    return mapping, state


def compose(earlier, latter):
    both = left_exact(latter[0], jnp.concatenate(earlier, axis=1))
    n = 2 * WIDTH
    return both[:, :n], both[:, n:] + latter[1]


def folded(slots, count, position):
    n = 2 * WIDTH
    eye = jnp.where(iota((n, n), 0) == iota((n, n), 1), 1.0, 0.0)
    before = (eye, jnp.zeros((n, n), f32))
    total = unpacked(slots[0])
    for k in range(1, count):
        hit = position == k
        before = tuple(jnp.where(hit, new, old) for new, old in zip(total, before))
        total = compose(total, unpacked(slots[k]))
    return before, total


def block_inverse(strict, found, first, end):
    n = strict.shape[0]
    row, col = iota((n, n), 0), iota((n, n), 1)
    if found is None:
        found = jnp.where(row == col, 1.0, 0.0) + jnp.where(row // 2 == col // 2, strict, 0.0)
    m = first
    while m < end:
        edge = jnp.where((row // (2 * m) == col // (2 * m)) & (row // m != col // m), strict, 0.0)
        found = found + fine(found, fine(edge, found))
        m *= 2
    return found


def mixer_start(r_ref, k_ref, v_ref, fade_ref, rate_ref):
    r, k, v = r_ref[...].astype(f32), k_ref[...].astype(f32), v_ref[...].astype(f32)
    n = r.shape[0]
    row, col = iota((n, n), 0), iota((n, n), 1)
    ones = jnp.where(head_blocks(n), 1.0, 0.0)
    log_fade = -jax.nn.sigmoid(fade_ref[...]) * 0.6065306597126334
    total_log = left_exact(jnp.where(row >= col, 1.0, 0.0), log_fade)
    length = jnp.sqrt(right_exact(k * k, ones))
    unit = k / jnp.maximum(length, 1.0)
    amount = unit * jax.nn.sigmoid(rate_ref[...])
    kept = jnp.exp(total_log)
    grown = jnp.exp(-total_log)
    erase = -unit * jnp.exp(total_log - log_fade)
    read = r * kept
    amount_grown, key_grown = amount * grown, k * grown
    last = kept[n - 1 :, :]
    right = jnp.concatenate([amount_grown, key_grown], axis=0)
    heads = []
    for h in range(n // WIDTH):
        mine = col // WIDTH == h
        erase_h = jnp.where(mine, erase, 0.0)
        read_h = jnp.where(mine, read, 0.0)
        grams = fine(jnp.concatenate([erase_h, read_h], axis=0), right, NT)
        within = jnp.where(row > col, grams[:n, :n], 0.0)
        heads.append((erase_h, grams, within, block_inverse(within, None, 2, SPLIT)))
    return v, read, last, amount_grown, key_grown, heads


def mixer_end(v, read, last, amount_grown, key_grown, heads):
    n = v.shape[0]
    row, col = iota((n, n), 0), iota((n, n), 1)
    strict, lower = row > col, row >= col
    maps = jnp.zeros((n, n), f32)
    values = jnp.zeros((n, n), f32)
    probe, local_out = read, jnp.zeros((n, n), f32)
    for h, (erase_h, grams, within, inverse) in enumerate(heads):
        value_h = jnp.where(col // WIDTH == h, v, 0.0)
        inverse = block_inverse(within, inverse, SPLIT, n)
        pushed = fine(jnp.where(strict, grams[:n, n:], 0.0), value_h)
        solved = fine(inverse, jnp.concatenate([erase_h, pushed], axis=1))
        shown = fine(jnp.where(lower, grams[n:, :n], 0.0), solved)
        local_out = local_out + shown[:, n:]
        local_out = local_out + fine(jnp.where(lower, grams[n:, n:], 0.0), value_h)
        probe = probe + shown[:, :n]
        maps = maps + solved[:, :n]
        values = values + solved[:, n:]
    same = head_blocks(n)
    amount_end, key_end = amount_grown * last, key_grown * last
    mapping = jnp.where(row == col, last, 0.0) + jnp.where(same, fine(amount_end, maps, TN), 0.0)
    state = jnp.where(same, fine(amount_end, values, TN) + fine(key_end, v, TN), 0.0)
    return mapping, state, probe, local_out


def layer_kernel(
    nz, ny, nt, span, inputs, *refs,
):
    given, out_ref, held = refs[:inputs], refs[inputs], refs[inputs + 1 : 2 * inputs + 1]
    load_sem, rest = refs[2 * inputs + 1], refs[2 * inputs + 2 :]
    (
        r_ref, k_ref, v_ref, fade_ref, rate_ref, switch_ref, bonus_ref, rescale_ref,
        exit_ref, skip_ref, scaling_ref, gate_ref, up_ref, taps_ref, down_ref,
    ) = held
    loads = [
        pltpu.make_async_copy(source, target, load_sem.at[i])
        for i, (source, target) in enumerate(zip(given, held))
    ]
    first_loads, second_loads = [3, 1, 4, 0, 2], [11, 12, 14]
    last_loads = [i for i in range(inputs) if i not in first_loads + second_loads]
    for i in first_loads + second_loads + last_loads:
        loads[i].start()
    (
    full_ref, near, mid, far, pieces, parts, probe_ref, local_ref, before_ref, carry_ref,
    sent, landed, stream_ref, rows_ref, gate_scr, edge_out, edge_in, partial, swapped, summed,
    first, second, final, gate_rows_ref, up_rows_ref,
    token_sem, near_send, near_recv, mid_send, mid_recv, far_send, far_recv, part_send, part_recv,
    plus_send, plus_recv, minus_send, minus_recv,
    exit_send, exit_recv, one_send, one_recv, two_send, two_recv, pair_send, pair_recv,
    edge_send, edge_recv, swap_send, swap_recv, first_send, first_recv, last_send, last_recv,
    ) = rest
    z, y, t = lax.axis_index("sp_0"), lax.axis_index("sp_1"), lax.axis_index("tp")
    nx = nt // 2
    x, core = t // 2, lax.rem(t, 2)
    groups = nz // span
    inner, outer = lax.rem(z, span), z // span
    n = 2 * WIDTH
    units = full_ref.shape[1]
    rows = gate_ref.shape[0]

    def along_y(j):
        return {"sp_1": ring_index(y, j, ny)}

    def along_z(to):
        return {"sp_0": to}

    barrier = pltpu.get_barrier_semaphore()
    for j in range(1, ny):
        pl.semaphore_signal(barrier, inc=1, device_id=along_y(j), device_id_type=MESH)
    reach = sorted({j % nz for j in range(-span, span + 1)} - {0})
    for j in reach:
        pl.semaphore_signal(
            barrier, inc=1, device_id=along_z(ring_index(z, j, nz)), device_id_type=MESH
        )
    for j in range(1, nt):
        pl.semaphore_signal(
            barrier, inc=1, device_id={"tp": ring_index(t, j, nt)}, device_id_type=MESH
        )

    for i in first_loads:
        loads[i].wait()
    begun = mixer_start(r_ref, k_ref, v_ref, fade_ref, rate_ref)

    for i in second_loads:
        loads[i].wait()
    stacked = jnp.concatenate([gate_ref[...], up_ref[...], down_ref[...]], axis=0)
    wide = pieces.shape[2]
    tall = stacked.shape[1]
    for part in range(ny):
        at, to = iota((tall, wide), 0), iota((tall, wide), 1)
        pick = jnp.where((at == to + part * units) & (to < units), 1.0, 0.0).astype(bf16)
        pieces[part] = plain(stacked, pick).astype(bf16)

    for i in last_loads:
        loads[i].wait()
    pl.semaphore_wait(barrier, ny - 1 + len(reach) + nt - 1)
    if nz > 2 * span:
        pl.semaphore_signal(
            token_sem, inc=1, device_id=along_z(ring_index(z, -span, nz)), device_id_type=MESH
        )

    def near_copy(source, target):
        return pltpu.make_async_remote_copy(
            src_ref=near.at[source], dst_ref=near.at[source],
            send_sem=near_send.at[target], recv_sem=near_recv.at[target],
            device_id=along_y(target), device_id_type=MESH,
        )

    def part_copy(j, arriving):
        to = ring_index(y, j, ny)
        source = ring_index(y, -j, ny) if arriving else y
        return pltpu.make_async_remote_copy(
            src_ref=pieces.at[to], dst_ref=parts.at[source],
            send_sem=part_send.at[j], recv_sem=part_recv.at[j],
            device_id=along_y(j), device_id_type=MESH,
        )

    for j in range(1, ny):
        part_copy(j, False).start()
    parts[y] = pieces[y]

    mapping, state, probe, local_out = mixer_end(*begun)
    near[y] = packed(mapping, state)
    for j in range(1, ny):
        near_copy(y, j).start()
    probe_ref[...] = probe
    local_ref[...] = local_out

    for j in range(1, ny):
        part_copy(j, True).wait_recv()
    square = jnp.where(iota((units, wide), 0) == iota((units, wide), 1), 1.0, 0.0).astype(bf16)
    for c in range(3):
        tallest = jnp.concatenate(
            [parts[part, c * rows : (c + 1) * rows, :] for part in range(ny)], axis=0
        )
        block = plain(square, tallest, NT).astype(bf16)
        full_ref[c, :, pl.ds(pl.multiple_of(z * ny * rows, ny * rows), ny * rows)] = block

    def piece(c, at):
        return full_ref.at[c, :, pl.ds(pl.multiple_of(at * ny * rows, ny * rows), ny * rows)]

    def plus_copy(c, s, at):
        return pltpu.make_async_remote_copy(
            src_ref=piece(c, at), dst_ref=piece(c, at),
            send_sem=plus_send.at[c, s], recv_sem=plus_recv.at[c, s],
            device_id=along_z(ring_index(z, 1, nz)), device_id_type=MESH,
        )

    def minus_copy(c, s, at):
        return pltpu.make_async_remote_copy(
            src_ref=piece(c, at), dst_ref=piece(c, at),
            send_sem=minus_send.at[c, s], recv_sem=minus_recv.at[c, s],
            device_id=along_z(ring_index(z, -1, nz)), device_id_type=MESH,
        )

    n_plus = nz // 2
    n_minus = nz - 1 - n_plus

    def ring_step(s):
        for c in range(3):
            if s > 0 and s <= n_plus:
                plus_copy(c, s - 1, ring_index(z, -s, nz)).wait_recv()
            if s < n_plus:
                plus_copy(c, s, ring_index(z, -s, nz)).start()
            if s > 0 and s <= n_minus:
                minus_copy(c, s - 1, ring_index(z, s, nz)).wait_recv()
            if s < n_minus:
                minus_copy(c, s, ring_index(z, s, nz)).start()

    ring_step(0)
    pending = list(range(1, n_plus + 1))

    def ring_steps(count):
        for s in pending[:count]:
            ring_step(s)
        del pending[:count]

    for j in range(1, ny):
        near_copy(ring_index(y, -j, ny), j).wait_recv()
    before, total = folded(near, ny, y)
    before_ref[0] = before[0]
    before_ref[1] = before[1]

    def mid_copy(source, j):
        to = z - inner + ring_index(inner, j, span)
        return pltpu.make_async_remote_copy(
            src_ref=mid.at[source], dst_ref=mid.at[source],
            send_sem=mid_send.at[j], recv_sem=mid_recv.at[j],
            device_id=along_z(to), device_id_type=MESH,
        )

    mid[inner] = packed(*total)
    for j in range(1, span):
        mid_copy(inner, j).start()

    ring_steps(FIRST)
    for j in range(1, span):
        mid_copy(ring_index(inner, -j, span), j).wait_recv()
    before_z, total_z = folded(mid, span, inner)
    before_ref[2] = before_z[0]
    before_ref[3] = before_z[1]

    def far_copy(slot, d, to):
        return pltpu.make_async_remote_copy(
            src_ref=far.at[slot], dst_ref=far.at[slot],
            send_sem=far_send.at[d], recv_sem=far_recv.at[d],
            device_id=along_z(to), device_id_type=MESH,
        )

    far[outer] = packed(*total_z)
    if nz > 2 * span:
        pl.semaphore_wait(token_sem, 1)
    for d in range(1, groups):
        @pl.when(outer + d < groups)
        def _():
            far_copy(outer, d, lax.rem(z + d * span, nz)).start()

    ring_steps(SECOND)

    carry_ref[...] = jnp.zeros((n, n), f32)
    for g in range(groups - 1):
        @pl.when(outer > g)
        def _():
            for d in range(1, groups):
                @pl.when(outer - g == d)
                def _():
                    far_copy(g, d, lax.rem(z + d * span, nz)).wait_recv()
            step = unpacked(far[g])
            carry_ref[...] = left_exact(step[0], carry_ref[...]) + step[1]
    incoming = fine(before_ref[2], carry_ref[...]) + before_ref[3]
    incoming = fine(before_ref[0], incoming) + before_ref[1]

    closing = local_ref[...] + fine(probe_ref[...], incoming)
    ones = jnp.where(head_blocks(n), 1.0, 0.0)
    centred = closing - right_exact(closing, ones) * (1.0 / WIDTH)
    spread = right_exact(centred * centred, ones) * (1.0 / WIDTH)
    rescaled = centred * lax.rsqrt(spread + group_eps) * rescale_ref[...]
    value = v_ref[...].astype(f32)
    bonus = right_exact(r_ref[...].astype(f32) * k_ref[...].astype(f32) * bonus_ref[...], ones)
    bonus = bonus * value
    mixed = ((rescaled + bonus) * switch_ref[...].astype(f32)).astype(bf16)

    own = n // nt
    width = exit_ref.shape[1]

    def exit_copy(j):
        to = ring_index(t, j, nt)
        return pltpu.make_async_remote_copy(
            src_ref=sent.at[to], dst_ref=landed.at[j],
            send_sem=exit_send.at[j], recv_sem=exit_recv.at[j],
            device_id={"tp": to}, device_id_type=MESH,
        )

    sent[...] = plain(mixed, exit_ref[...]).astype(bf16).reshape(nt, own, width)
    for j in range(1, nt):
        exit_copy(j).start()
    ring_steps(MIDDLE)
    attended = sent[t].astype(f32)
    for j in range(1, nt):
        exit_copy(j).wait_recv()
    for j in range(1, nt):
        attended = attended + landed[j].astype(f32)
    stream = skip_ref[...].astype(f32) + attended
    stream_ref[...] = stream
    mean = jnp.mean(stream * stream, axis=-1, keepdims=True)
    rows_ref[y, x, core] = (stream * lax.rsqrt(mean + norm_eps) * scaling_ref[...]).astype(bf16)

    across = 1 - core
    na = ny
    a, b = y * across + x * core, x * across + y * core

    def place(a_to, b_to):
        return a_to * across + b_to * core, b_to * across + a_to * core

    def device(a_to, b_to):
        y_to, x_to = place(a_to, b_to)
        return {"sp_1": y_to, "tp": 2 * x_to + core}

    def slot(j, i):
        y_at, x_at = place(ring_index(a, -j, na), ring_index(b, -i, na))
        return rows_ref.at[y_at, x_at, core]

    def one_copy(j, arriving):
        ref = slot(0, j if arriving else 0)
        return pltpu.make_async_remote_copy(
            src_ref=ref, dst_ref=ref, send_sem=one_send.at[j], recv_sem=one_recv.at[j],
            device_id=device(a, ring_index(b, j, na)), device_id_type=MESH,
        )

    def two_copy(j, i, arriving):
        ref = slot(j if arriving else 0, i)
        return pltpu.make_async_remote_copy(
            src_ref=ref, dst_ref=ref, send_sem=two_send.at[j, i], recv_sem=two_recv.at[j, i],
            device_id=device(ring_index(a, j, na), b), device_id_type=MESH,
        )

    partner = {"tp": t + 1 - 2 * core}

    def pair_copy(j, i, arriving):
        if arriving:
            y_at, x_at = place(ring_index(a, -i, na), ring_index(b, -j, na))
            ref = rows_ref.at[y_at, x_at, 1 - core]
        else:
            ref = slot(j, i)
        return pltpu.make_async_remote_copy(
            src_ref=ref, dst_ref=ref, send_sem=pair_send.at[j, i], recv_sem=pair_recv.at[j, i],
            device_id=partner, device_id_type=MESH,
        )

    for j in range(1, na):
        one_copy(j, False).start()
    for j in range(1, na):
        two_copy(j, 0, False).start()
    pair_copy(0, 0, False).start()
    ring_steps(LATE)
    for i in range(1, na):
        one_copy(i, True).wait_recv()
        for j in range(1, na):
            two_copy(j, i, False).start()
        pair_copy(0, i, False).start()
    ring_steps(len(pending))
    units_at = iota((taps_ref.shape[1], units), 0) == iota((taps_ref.shape[1], units), 1) + y * units
    taps = exact(taps_ref[...], jnp.where(units_at, 1.0, 0.0))
    for i in range(na):
        for j in range(1, na):
            two_copy(j, i, True).wait_recv()
            pair_copy(j, i, False).start()
    tokens = na * n
    half = tokens // 2

    def projections(c):
        rows = rows_ref[:, :, c].reshape(half, width)
        gate_rows_ref[:, :, c] = plain(rows, full_ref[0], NT).reshape(ny, nx, own, units)
        up_rows_ref[:, :, c] = plain(rows, full_ref[1], NT).reshape(ny, nx, own, units)

    projections(core)
    for i in range(na):
        for j in range(na):
            pair_copy(j, i, True).wait_recv()
    projections(1 - core)
    gate_pre = gate_rows_ref[...].reshape(tokens, units).astype(bf16)
    edge = edge_out.shape[0]
    edge_out[...] = gate_pre[tokens - edge :, :]

    def edge_copy():
        return pltpu.make_async_remote_copy(
            src_ref=edge_out, dst_ref=edge_in, send_sem=edge_send.at[0], recv_sem=edge_recv.at[0],
            device_id=along_z(ring_index(z, 1, nz)), device_id_type=MESH,
        )

    @pl.when(z < nz - 1)
    def _():
        edge_copy().start()

    gate_scr[edge:, :] = gate_pre.astype(f32)
    up_part = up_rows_ref[...].reshape(tokens, units).astype(bf16)

    @pl.when(z > 0)
    def _():
        edge_copy().wait_recv()
        gate_scr[:edge, :] = edge_in[...].astype(f32)

    @pl.when(z == 0)
    def _():
        gate_scr[:edge, :] = jnp.zeros((edge, units), f32)

    count = taps_ref.shape[0]
    conv = jnp.zeros((tokens, units), f32)
    for tap in range(count):
        start = edge - count + 1 + tap
        conv = conv + taps[tap : tap + 1, :] * gate_scr[start : start + tokens, :]
    hidden = (conv / (1.0 + jnp.exp(-conv)) * up_part.astype(f32)).astype(bf16)

    bands = partial.shape[0]
    band = width // bands

    def swap_copy(p):
        return pltpu.make_async_remote_copy(
            src_ref=partial.at[p, :, :, 1 - core], dst_ref=swapped.at[p],
            send_sem=swap_send.at[p], recv_sem=swap_recv.at[p],
            device_id=partner, device_id_type=MESH,
        )

    def first_copy(p, j):
        return pltpu.make_async_remote_copy(
            src_ref=summed.at[p, ring_index(a, j, na)], dst_ref=first.at[p, j],
            send_sem=first_send.at[p, j], recv_sem=first_recv.at[p, j],
            device_id=device(ring_index(a, j, na), b), device_id_type=MESH,
        )

    def last_copy(p, j):
        return pltpu.make_async_remote_copy(
            src_ref=second.at[p, ring_index(b, j, na)], dst_ref=final.at[p, j],
            send_sem=last_send.at[p, j], recv_sem=last_recv.at[p, j],
            device_id=device(a, ring_index(b, j, na)), device_id_type=MESH,
        )

    for p in range(bands):
        product = plain(hidden, full_ref[2, :, p * band : (p + 1) * band]).astype(bf16)
        partial[p] = product.reshape(ny, nx, 2, own, band)
        swap_copy(p).start()
    order = list(range(1, na)) + [0]
    for p in range(bands):
        swap_copy(p).wait_recv()
        for j in order:
            a_to = ring_index(a, j, na)
            for b_to in range(na):
                y_at, x_at = place(a_to, b_to)
                both = partial[p, y_at, x_at, core].astype(f32)
                both = both + swapped[p, y_at, x_at].astype(f32)
                summed[p, a_to, b_to] = both.astype(bf16)
            if j > 0:
                first_copy(p, j).start()
    for p in range(bands):
        for j in range(1, na):
            first_copy(p, j).wait_recv()
        for j in order:
            b_to = ring_index(b, j, na)
            total_rows = summed[p, a, b_to].astype(f32)
            for i in range(1, na):
                total_rows = total_rows + first[p, i, b_to].astype(f32)
            second[p, b_to] = total_rows.astype(bf16)
            if j > 0:
                last_copy(p, j).start()
    for p in range(bands):
        projected = second[p, b].astype(f32)
        for j in range(1, na):
            last_copy(p, j).wait_recv()
        for j in range(1, na):
            projected = projected + final[p, j].astype(f32)
        columns = slice(p * band, (p + 1) * band)
        out_ref[:, columns] = (stream_ref[:, columns] + projected).astype(bf16)

    for j in range(1, ny):
        near_copy(y, j).wait_send()
        part_copy(j, False).wait_send()
    for j in range(1, span):
        mid_copy(inner, j).wait_send()
    for d in range(1, groups):
        @pl.when(outer + d < groups)
        def _():
            far_copy(outer, d, lax.rem(z + d * span, nz)).wait_send()
    for c in range(3):
        for s in range(n_plus):
            plus_copy(c, s, ring_index(z, -s, nz)).wait_send()
        for s in range(n_minus):
            minus_copy(c, s, ring_index(z, s, nz)).wait_send()
    for j in range(1, nt):
        exit_copy(j).wait_send()
    for j in range(1, na):
        one_copy(j, False).wait_send()
        for p in range(bands):
            first_copy(p, j).wait_send()
            last_copy(p, j).wait_send()
        for i in range(na):
            two_copy(j, i, False).wait_send()
    for i in range(na):
        for j in range(na):
            pair_copy(j, i, False).wait_send()
    for p in range(bands):
        swap_copy(p).wait_send()

    @pl.when(z < nz - 1)
    def _():
        edge_copy().wait_send()


def layer(*args):
    r, skip, gate = args[0], args[9], args[11]
    nz, ny, nt = lax.axis_size("sp_0"), lax.axis_size("sp_1"), lax.axis_size("tp")
    span = min(4, nz)
    groups = nz // span
    nx = nt // 2
    n = r.shape[0]
    rows, hidden = gate.shape
    units = hidden // ny
    wide = -(-units // 128) * 128
    own, width = skip.shape
    band = width // BANDS
    dma = pltpu.SemaphoreType.DMA
    in_vmem = pl.BlockSpec(memory_space=pltpu.VMEM)
    n_plus = nz // 2
    edge = 16
    return pl.pallas_call(
        functools.partial(layer_kernel, nz, ny, nt, span, len(args)),
        out_shape=jax.ShapeDtypeStruct((own, width), bf16),
        in_specs=[pl.BlockSpec(memory_space=pl.ANY)] * len(args),
        out_specs=in_vmem,
        scratch_shapes=[pltpu.VMEM(arg.shape, arg.dtype) for arg in args]
        + [
            dma((len(args),)),
            pltpu.VMEM((3, units, nz * ny * rows), bf16),
            pltpu.VMEM((ny, n, n), bf16),
            pltpu.VMEM((span, n, n), bf16),
            pltpu.VMEM((groups, n, n), bf16),
            pltpu.VMEM((ny, 3 * rows, wide), bf16),
            pltpu.VMEM((ny, 3 * rows, wide), bf16),
            pltpu.VMEM((n, n), f32),
            pltpu.VMEM((n, n), f32),
            pltpu.VMEM((4, n, n), f32),
            pltpu.VMEM((n, n), f32),
            pltpu.VMEM((nt, own, width), bf16),
            pltpu.VMEM((nt, own, width), bf16),
            pltpu.VMEM((own, width), f32),
            pltpu.VMEM((ny, nx, 2, own, width), bf16),
            pltpu.VMEM((edge + ny * n, units), f32),
            pltpu.VMEM((edge, units), bf16),
            pltpu.VMEM((edge, units), bf16),
            pltpu.VMEM((BANDS, ny, nx, 2, own, band), bf16),
            pltpu.VMEM((BANDS, ny, nx, own, band), bf16),
            pltpu.VMEM((BANDS, ny, nx, own, band), bf16),
            pltpu.VMEM((BANDS, ny, nx, own, band), bf16),
            pltpu.VMEM((BANDS, nx, own, band), bf16),
            pltpu.VMEM((BANDS, nx, own, band), bf16),
            pltpu.VMEM((ny, nx, 2, own, units), f32),
            pltpu.VMEM((ny, nx, 2, own, units), f32),
            pltpu.SemaphoreType.REGULAR,
            dma((ny,)), dma((ny,)), dma((span,)), dma((span,)), dma((groups,)), dma((groups,)),
            dma((ny,)), dma((ny,)),
            dma((3, n_plus)), dma((3, n_plus)), dma((3, n_plus)), dma((3, n_plus)),
            dma((nt,)), dma((nt,)), dma((nx,)), dma((nx,)),
            dma((ny, nx)), dma((ny, nx)), dma((ny, nx)), dma((ny, nx)),
            dma((1,)), dma((1,)), dma((BANDS,)), dma((BANDS,)),
            dma((BANDS, ny)), dma((BANDS, ny)), dma((BANDS, nx)), dma((BANDS, nx)),
        ],
        compiler_params=pltpu.CompilerParams(
            collective_id=0, has_side_effects=True, vmem_limit_bytes=67043328
        ),
        name="layer",
    )(*args)


def body(
    r, k, v, fade, rate, switch, bonus, rescale, leave, skip, scaling, gate, up, taps, down
):
    return layer(
        r, k, v, fade, rate, switch, bonus[None], rescale[None], leave, skip, scaling[None],
        gate, up, taps, down.T,
    )


def solution(mesh):
    sp, tp = mesh.shape["sp"], mesh.shape["tp"]
    ny = COLUMNS
    finer = Mesh(mesh.devices.reshape(sp // ny, ny, tp), SP_TP)
    cut = P(SP, "tp")
    placed = (
        cut, cut, cut, cut, cut, cut, P("tp"), P("tp"), P("tp", None), P(SP_TP, None), P(),
        cut, cut, P(None, "tp"), P("tp", SP),
    )
    return jax.shard_map(
        body, mesh=finer, in_specs=placed, out_specs=P(SP_TP, None), check_vma=False
    )
```

```python
import functools

import jax
import jax.numpy as jnp
from jax import lax
from jax.experimental import pallas as pl
from jax.experimental.pallas import tpu as pltpu
from jax.sharding import Mesh
from jax.sharding import PartitionSpec as P

WIDTH = 64
SP = ("sp_0", "sp_1")
SP_TP = ("sp_0", "sp_1", "tp")
COLUMNS = 4
BANDS = 4
SPLIT = 16
MIX, LATER, LESS = 0, 2, 1
MESH = pl.DeviceIdType.MESH

group_eps = 0.00064
norm_eps = 1e-06
f32 = jnp.float32
bf16 = jnp.bfloat16

NN = (((1,), (0,)), ((), ()))
NT = (((1,), (1,)), ((), ()))
TN = (((0,), (0,)), ((), ()))


def exact(a, b, dims=NN):
    return lax.dot_general(
        a, b, dims, precision=lax.Precision.HIGHEST, preferred_element_type=f32
    )


def plain(a, b, dims=NN):
    return lax.dot_general(a, b, dims, preferred_element_type=f32)


def split(a):
    high = a.astype(bf16)
    return high, (a - high.astype(f32)).astype(bf16)


def fine(a, b, dims=NN):
    (a_dim,), (b_dim,) = dims[0]
    a_high, a_low = split(a)
    b_high, b_low = split(b)
    left = jnp.concatenate([a_high, a_high, a_low], axis=a_dim)
    right = jnp.concatenate([b_high, b_low, b_high], axis=b_dim)
    return plain(left, right, dims)


def left_exact(a, b):
    a = a.astype(bf16)
    return plain(jnp.concatenate([a, a], axis=1), jnp.concatenate(split(b), axis=0))


def right_exact(a, b):
    b = b.astype(bf16)
    return plain(jnp.concatenate(split(a), axis=1), jnp.concatenate([b, b], axis=0))


def iota(shape, dim):
    return lax.broadcasted_iota(jnp.int32, shape, dim)


def ring_index(base, step, size):
    return lax.rem(base + step + size, size)


def head_blocks(n):
    return (iota((n, n), 0) // WIDTH) == (iota((n, n), 1) // WIDTH)


def packed(mapping, state):
    return jnp.concatenate(
        [mapping[:WIDTH] + mapping[WIDTH:], state[:WIDTH] + state[WIDTH:]], axis=0
    ).astype(bf16)


def unpacked_half(half):
    half = half.astype(f32)
    return jnp.where(head_blocks(2 * WIDTH), jnp.concatenate([half, half], axis=0), 0.0)


def unpacked(block):
    return unpacked_half(block[:WIDTH]), unpacked_half(block[WIDTH:])


def compose(earlier, latter):
    both = left_exact(latter[0], jnp.concatenate(earlier, axis=1))
    n = 2 * WIDTH
    return both[:, :n], both[:, n:] + latter[1]


def folded(slots, heads, count, position):
    n = 2 * WIDTH
    eye = jnp.where(iota((n, n), 0) == iota((n, n), 1), 1.0, 0.0)
    before = (eye, jnp.zeros((n, n), f32))
    total = unpacked(slots[0, heads])
    for k in range(1, count):
        hit = position == k
        before = tuple(jnp.where(hit, new, old) for new, old in zip(total, before))
        total = compose(total, unpacked(slots[k, heads]))
    return before, total


def block_inverse(strict, found, first, end):
    n = strict.shape[0]
    row, col = iota((n, n), 0), iota((n, n), 1)
    if found is None:
        found = jnp.where(row == col, 1.0, 0.0) + jnp.where(row // 2 == col // 2, strict, 0.0)
    m = first
    while m < end:
        edge = jnp.where((row // (2 * m) == col // (2 * m)) & (row // m != col // m), strict, 0.0)
        found = found + fine(found, fine(edge, found))
        m *= 2
    return found


def mixer_start(r_ref, k_ref, v_ref, fade_ref, rate_ref):
    r, k, v = r_ref[...].astype(f32), k_ref[...].astype(f32), v_ref[...].astype(f32)
    n = r.shape[0]
    row, col = iota((n, n), 0), iota((n, n), 1)
    ones = jnp.where(head_blocks(n), 1.0, 0.0)
    log_fade = -jax.nn.sigmoid(fade_ref[...]) * 0.6065306597126334
    total_log = left_exact(jnp.where(row >= col, 1.0, 0.0), log_fade)
    length = jnp.sqrt(right_exact(k * k, ones))
    unit = k / jnp.maximum(length, 1.0)
    amount = unit * jax.nn.sigmoid(rate_ref[...])
    kept = jnp.exp(total_log)
    grown = jnp.exp(-total_log)
    erase = -unit * jnp.exp(total_log - log_fade)
    read = r * kept
    amount_grown, key_grown = amount * grown, k * grown
    last = kept[n - 1 :, :]
    right = jnp.concatenate([amount_grown, key_grown], axis=0)
    heads = []
    for h in range(n // WIDTH):
        mine = col // WIDTH == h
        erase_h = jnp.where(mine, erase, 0.0)
        read_h = jnp.where(mine, read, 0.0)
        grams = fine(jnp.concatenate([erase_h, read_h], axis=0), right, NT)
        within = jnp.where(row > col, grams[:n, :n], 0.0)
        heads.append((erase_h, grams, within, block_inverse(within, None, 2, SPLIT)))
    return v, read, last, amount_grown, key_grown, heads


def mixer_end(v, read, last, amount_grown, key_grown, heads):
    n = v.shape[0]
    row, col = iota((n, n), 0), iota((n, n), 1)
    strict, lower = row > col, row >= col
    maps = jnp.zeros((n, n), f32)
    values = jnp.zeros((n, n), f32)
    probe, local_out = read, jnp.zeros((n, n), f32)
    for h, (erase_h, grams, within, inverse) in enumerate(heads):
        value_h = jnp.where(col // WIDTH == h, v, 0.0)
        inverse = block_inverse(within, inverse, SPLIT, n)
        pushed = fine(jnp.where(strict, grams[:n, n:], 0.0), value_h)
        solved = fine(inverse, jnp.concatenate([erase_h, pushed], axis=1))
        shown = fine(jnp.where(lower, grams[n:, :n], 0.0), solved)
        local_out = local_out + shown[:, n:]
        local_out = local_out + fine(jnp.where(lower, grams[n:, n:], 0.0), value_h)
        probe = probe + shown[:, :n]
        maps = maps + solved[:, :n]
        values = values + solved[:, n:]
    same = head_blocks(n)
    amount_end, key_end = amount_grown * last, key_grown * last
    mapping = jnp.where(row == col, last, 0.0) + jnp.where(same, fine(amount_end, maps, TN), 0.0)
    state = jnp.where(same, fine(amount_end, values, TN) + fine(key_end, v, TN), 0.0)
    return mapping, state, probe, local_out


def layer_kernel(
    nz, ny, nt, span, inputs, *refs,
):
    given, out_ref, held = refs[:inputs], refs[inputs], refs[inputs + 1 : 2 * inputs + 1]
    load_sem, rest = refs[2 * inputs + 1], refs[2 * inputs + 2 :]
    (
        r_ref, k_ref, v_ref, fade_ref, rate_ref, switch_ref, bonus_ref, rescale_ref,
        exit_ref, skip_ref, scaling_ref, gate_ref, up_ref, taps_ref, down_ref,
    ) = held
    loads = [
        pltpu.make_async_copy(source, target, load_sem.at[i])
        for i, (source, target) in enumerate(zip(given, held))
    ]
    first_loads, second_loads = [3, 1, 4, 0, 2], [11, 12, 14]
    last_loads = [i for i in range(inputs) if i not in first_loads + second_loads]
    for i in first_loads + second_loads + last_loads:
        loads[i].start()
    (
    full_ref, near, mid, far, pieces, parts, finish_ref, before_ref, carry_ref, exit_both,
    sent, landed, stream_ref, rows_ref, gate_scr, edge_out, edge_in, partial, swapped, summed,
    first, second, final, gate_rows_ref, up_rows_ref,
    token_sem, near_send, near_recv, mid_send, mid_recv, far_send, far_recv, part_send, part_recv,
    plus_send, plus_recv, minus_send, minus_recv,
    finish_send, finish_recv, twin_send, twin_recv, hand_send, hand_recv,
    exit_send, exit_recv, one_send, one_recv, two_send, two_recv, pair_send, pair_recv,
    edge_send, edge_recv, swap_send, swap_recv, first_send, first_recv, last_send, last_recv,
    ) = rest
    z, y, t = lax.axis_index("sp_0"), lax.axis_index("sp_1"), lax.axis_index("tp")
    nx = nt // 2
    x, core = t // 2, lax.rem(t, 2)
    groups = nz // span
    inner, outer = lax.rem(z, span), z // span
    n = 2 * WIDTH
    units = full_ref.shape[2]
    rows = gate_ref.shape[0]

    def along_y(j):
        return {"sp_1": ring_index(y, j, ny)}

    def along_z(to):
        return {"sp_0": to}

    mixes = core == MIX
    forwards = core == 1 - MIX
    head_set = jnp.where(mixes, 0, 1)
    chip = t - core
    mate = chip + 1 - core
    mixer_at, ring_at = chip + MIX, chip + 1 - MIX

    barrier = pltpu.get_barrier_semaphore()
    for j in range(1, ny):
        for to in (t, mate):
            pl.semaphore_signal(
                barrier, inc=1, device_id={"sp_1": ring_index(y, j, ny), "tp": to},
                device_id_type=MESH,
            )
    reach = sorted({j % nz for j in range(-span, span + 1)} - {0})
    for j in reach:
        pl.semaphore_signal(
            barrier, inc=1, device_id=along_z(ring_index(z, j, nz)), device_id_type=MESH
        )
    for j in range(1, nt):
        pl.semaphore_signal(
            barrier, inc=1, device_id={"tp": ring_index(t, j, nt)}, device_id_type=MESH
        )

    for i in first_loads:
        loads[i].wait()
    begun = mixer_start(r_ref, k_ref, v_ref, fade_ref, rate_ref)

    for i in second_loads:
        loads[i].wait()
    stacked = jnp.concatenate([gate_ref[...], up_ref[...], down_ref[...]], axis=0)
    wide = pieces.shape[2]
    tall = stacked.shape[1]
    for part in range(ny):
        at, to = iota((tall, wide), 0), iota((tall, wide), 1)
        pick = jnp.where((at == to + part * units) & (to < units), 1.0, 0.0).astype(bf16)
        pieces[part] = plain(stacked, pick).astype(bf16)

    for i in last_loads:
        loads[i].wait()
    pl.semaphore_wait(barrier, 2 * (ny - 1) + len(reach) + nt - 1)
    if nz > 2 * span:
        pl.semaphore_signal(
            token_sem, inc=1, device_id=along_z(ring_index(z, -span, nz)), device_id_type=MESH
        )

    def near_copy(source, j, heads):
        return pltpu.make_async_remote_copy(
            src_ref=near.at[source, heads], dst_ref=near.at[source, heads],
            send_sem=near_send.at[j], recv_sem=near_recv.at[j, heads],
            device_id={"sp_1": ring_index(y, j, ny), "tp": mixer_at}, device_id_type=MESH,
        )

    def part_copy(j, share):
        to = ring_index(y, j, ny)
        return pltpu.make_async_remote_copy(
            src_ref=pieces.at[to], dst_ref=parts.at[share, y],
            send_sem=part_send.at[j], recv_sem=part_recv.at[j, share],
            device_id={"sp_1": to, "tp": ring_at}, device_id_type=MESH,
        )

    def part_arrival(j, share):
        source = ring_index(y, -j, ny)
        return pltpu.make_async_remote_copy(
            src_ref=pieces.at[source], dst_ref=parts.at[share, source],
            send_sem=part_send.at[j], recv_sem=part_recv.at[j, share],
            device_id={"sp_1": source, "tp": ring_at}, device_id_type=MESH,
        )

    share = 1 - head_set
    for j in range(1, ny):
        part_copy(j, share).start()

    @pl.when(mixes)
    def _():
        part_copy(0, 1).start()

    @pl.when(forwards)
    def _():
        parts[0, y] = pieces[y]

    twin_copy = pltpu.make_async_remote_copy(
        src_ref=exit_ref, dst_ref=exit_both, send_sem=twin_send.at[0], recv_sem=twin_recv.at[0],
        device_id={"tp": mate}, device_id_type=MESH,
    )

    @pl.when(forwards)
    def _():
        twin_copy.start()

    mapping, state, probe, local_out = mixer_end(*begun)
    near[y, head_set] = packed(mapping, state)
    for j in range(1, ny):
        near_copy(y, j, head_set).start()

    @pl.when(forwards)
    def _():
        near_copy(y, 0, 1).start()

    ones = jnp.where(head_blocks(n), 1.0, 0.0)
    value, switch = v_ref[...].astype(f32), switch_ref[...].astype(f32)
    bonus = right_exact(r_ref[...].astype(f32) * k_ref[...].astype(f32) * bonus_ref[...], ones)
    finish_ref[head_set, 0] = probe
    finish_ref[head_set, 1] = local_out
    finish_ref[head_set, 2] = rescale_ref[...] * switch
    finish_ref[head_set, 3] = bonus * value * switch
    finish_copy = pltpu.make_async_remote_copy(
        src_ref=finish_ref.at[1], dst_ref=finish_ref.at[1],
        send_sem=finish_send.at[0], recv_sem=finish_recv.at[0],
        device_id={"tp": mate}, device_id_type=MESH,
    )

    @pl.when(forwards)
    def _():
        finish_copy.start()

    depth = ny * rows

    def piece(share, at):
        return full_ref.at[share, :, :, pl.ds(pl.multiple_of(at * depth, depth), depth)]

    def plus_copy(share, s, at):
        ref = piece(share, at)
        return pltpu.make_async_remote_copy(
            src_ref=ref, dst_ref=ref,
            send_sem=plus_send.at[share, s], recv_sem=plus_recv.at[share, s],
            device_id=along_z(ring_index(z, 1, nz)), device_id_type=MESH,
        )

    def minus_copy(share, s, at):
        ref = piece(share, at)
        return pltpu.make_async_remote_copy(
            src_ref=ref, dst_ref=ref,
            send_sem=minus_send.at[share, s], recv_sem=minus_recv.at[share, s],
            device_id=along_z(ring_index(z, -1, nz)), device_id_type=MESH,
        )

    def hand_copy(at, j):
        return pltpu.make_async_remote_copy(
            src_ref=piece(1, at), dst_ref=piece(0, at),
            send_sem=hand_send.at[j], recv_sem=hand_recv.at[j],
            device_id={"tp": mate}, device_id_type=MESH,
        )

    n_plus = max(1, nz // 2 - LESS) if nz > 2 else 1
    n_minus = nz - 1 - n_plus
    steps = max(n_plus, n_minus) + 1

    def ring_step(s):
        for share in range(2):
            after, ahead = ring_index(z, -s, nz), ring_index(z, s, nz)
            if s > 0 and s <= n_plus:
                plus_copy(share, s - 1, after).wait_recv()
            if s < n_plus:
                plus_copy(share, s, after).start()
            if s > 0 and s <= n_minus:
                minus_copy(share, s - 1, ahead).wait_recv()
            if s < n_minus:
                minus_copy(share, s, ahead).start()
            if share == 1:
                if s <= n_plus:
                    hand_copy(after, (nz - s) % nz).start()
                if s > 0 and s <= n_minus:
                    hand_copy(ahead, s).start()

    @pl.when(forwards)
    def _():
        for j in range(1, ny):
            for share in range(2):
                part_arrival(j, share).wait_recv()
        part_copy(0, 1).wait_recv()
        square = jnp.where(iota((units, wide), 0) == iota((units, wide), 1), 1.0, 0.0).astype(bf16)
        for share in range(2):
            for c in range(3):
                tallest = jnp.concatenate(
                    [parts[share, part, c * rows : (c + 1) * rows, :] for part in range(ny)], axis=0
                )
                block = plain(square, tallest, NT).astype(bf16)
                full_ref[share, c, :, pl.ds(pl.multiple_of(z * depth, depth), depth)] = block
        for s in range(max(0, steps - LATER)):
            ring_step(s)

    def later_ring_steps(first, end):
        todo = list(range(max(0, steps - LATER), steps))[first:end]
        if todo:
            @pl.when(forwards)
            def _():
                for s in todo:
                    ring_step(s)

    def mid_copy(source, j):
        to = z - inner + ring_index(inner, j, span)
        return pltpu.make_async_remote_copy(
            src_ref=mid.at[source], dst_ref=mid.at[source],
            send_sem=mid_send.at[j], recv_sem=mid_recv.at[j],
            device_id=along_z(to), device_id_type=MESH,
        )

    def far_copy(source, d, to, states_only):
        ref = far.at[source, 1] if states_only else far.at[source]
        return pltpu.make_async_remote_copy(
            src_ref=ref, dst_ref=ref, send_sem=far_send.at[d], recv_sem=far_recv.at[d],
            device_id=along_z(to), device_id_type=MESH,
        )

    def far_sends(action):
        for d in range(1, groups):
            to = lax.rem(z + d * span, nz)

            @pl.when(outer == 0)
            def _():
                getattr(far_copy(0, d, to, True), action)()

            @pl.when((outer > 0) & (outer + d < groups))
            def _():
                getattr(far_copy(outer, d, to, False), action)()

    def exit_copy(j, to_core):
        to = 2 * ring_index(x, j, nx) + to_core
        return pltpu.make_async_remote_copy(
            src_ref=sent.at[to], dst_ref=landed.at[j],
            send_sem=exit_send.at[j, to_core], recv_sem=exit_recv.at[j],
            device_id={"tp": to}, device_id_type=MESH,
        )

    own = n // nt
    width = exit_ref.shape[1]

    @pl.when(mixes)
    def _():
        for j in range(1, ny):
            for heads in range(2):
                near_copy(ring_index(y, -j, ny), j, heads).wait_recv()
        near_copy(y, 0, 1).wait_recv()
        totals = []
        for heads in range(2):
            before, total = folded(near, heads, ny, y)
            before_ref[heads, 0], before_ref[heads, 1] = before
            totals.append(packed(*total))
        for heads in range(2):
            mid[inner, heads] = totals[heads]
        for j in range(1, span):
            mid_copy(inner, j).start()
        for j in range(1, span):
            mid_copy(ring_index(inner, -j, span), j).wait_recv()
        totals = []
        for heads in range(2):
            before, total = folded(mid, heads, span, inner)
            before_ref[heads, 2], before_ref[heads, 3] = before
            totals.append(packed(*total))
        far[outer, 0] = jnp.concatenate([part[:WIDTH] for part in totals], axis=0)
        far[outer, 1] = jnp.concatenate([part[WIDTH:] for part in totals], axis=0)
        if nz > 2 * span:
            pl.semaphore_wait(token_sem, 1)
        far_sends("start")
        carry_ref[...] = jnp.zeros((2, n, n), f32)
        finish_copy.wait_recv()
        twin_copy.wait_recv()
        for g in range(groups - 1):
            @pl.when(outer > g)
            def _():
                for d in range(1, groups):
                    @pl.when(outer - g == d)
                    def _():
                        far_copy(g, d, lax.rem(z + d * span, nz), g == 0).wait_recv()
                for heads in range(2):
                    half = slice(heads * WIDTH, (heads + 1) * WIDTH)
                    state = unpacked_half(far[g, 1, half])
                    if g > 0:
                        state = state + left_exact(unpacked_half(far[g, 0, half]), carry_ref[heads])
                    carry_ref[heads] = state
        mixed = []
        for heads in range(2):
            incoming = fine(before_ref[heads, 2], carry_ref[heads]) + before_ref[heads, 3]
            incoming = fine(before_ref[heads, 0], incoming) + before_ref[heads, 1]
            closing = finish_ref[heads, 1] + fine(finish_ref[heads, 0], incoming)
            centred = closing - right_exact(closing, ones) * (1.0 / WIDTH)
            spread = right_exact(centred * centred, ones) * (1.0 / WIDTH)
            rescaled = centred * lax.rsqrt(spread + group_eps) * finish_ref[heads, 2]
            mixed.append((rescaled + finish_ref[heads, 3]).astype(bf16))
        product = plain(
            jnp.concatenate(mixed, axis=1), jnp.concatenate([exit_ref[...], exit_both[...]], axis=0)
        )
        sent[...] = product.astype(bf16).reshape(nt, own, width)
        for j in range(1, nx):
            for to_core in range(2):
                exit_copy(j, to_core).start()
        exit_copy(0, 1 - MIX).start()

    stream = skip_ref[...].astype(f32)
    for j in range(1, nx):
        exit_copy(j, core).wait_recv()

    @pl.when(mixes)
    def _():
        landed[0] = sent[t]

    @pl.when(forwards)
    def _():
        exit_copy(0, 1 - MIX).wait_recv()

    for j in range(nx):
        stream = stream + landed[j].astype(f32)
    stream_ref[...] = stream
    mean = jnp.mean(stream * stream, axis=-1, keepdims=True)
    rows_ref[y, x, core] = (stream * lax.rsqrt(mean + norm_eps) * scaling_ref[...]).astype(bf16)

    across = 1 - core
    na = ny
    a, b = y * across + x * core, x * across + y * core

    def place(a_to, b_to):
        return a_to * across + b_to * core, b_to * across + a_to * core

    def device(a_to, b_to):
        y_to, x_to = place(a_to, b_to)
        return {"sp_1": y_to, "tp": 2 * x_to + core}

    def slot(j, i):
        y_at, x_at = place(ring_index(a, -j, na), ring_index(b, -i, na))
        return rows_ref.at[y_at, x_at, core]

    def one_copy(j, arriving):
        ref = slot(0, j if arriving else 0)
        return pltpu.make_async_remote_copy(
            src_ref=ref, dst_ref=ref, send_sem=one_send.at[j], recv_sem=one_recv.at[j],
            device_id=device(a, ring_index(b, j, na)), device_id_type=MESH,
        )

    def two_copy(j, i, arriving):
        ref = slot(j if arriving else 0, i)
        return pltpu.make_async_remote_copy(
            src_ref=ref, dst_ref=ref, send_sem=two_send.at[j, i], recv_sem=two_recv.at[j, i],
            device_id=device(ring_index(a, j, na), b), device_id_type=MESH,
        )

    partner = {"tp": mate}

    def pair_copy(j, i, arriving):
        if arriving:
            y_at, x_at = place(ring_index(a, -i, na), ring_index(b, -j, na))
            ref = rows_ref.at[y_at, x_at, 1 - core]
        else:
            ref = slot(j, i)
        return pltpu.make_async_remote_copy(
            src_ref=ref, dst_ref=ref, send_sem=pair_send.at[j, i], recv_sem=pair_recv.at[j, i],
            device_id=partner, device_id_type=MESH,
        )

    for j in range(1, na):
        one_copy(j, False).start()
    for j in range(1, na):
        two_copy(j, 0, False).start()
    pair_copy(0, 0, False).start()
    later_ring_steps(0, 1)
    for i in range(1, na):
        one_copy(i, True).wait_recv()
        for j in range(1, na):
            two_copy(j, i, False).start()
        pair_copy(0, i, False).start()
    later_ring_steps(1, LATER)
    units_at = iota((taps_ref.shape[1], units), 0) == iota((taps_ref.shape[1], units), 1) + y * units
    taps = exact(taps_ref[...], jnp.where(units_at, 1.0, 0.0))
    for i in range(na):
        for j in range(1, na):
            two_copy(j, i, True).wait_recv()
            pair_copy(j, i, False).start()
    tokens = na * n
    half = tokens // 2

    def projections(c):
        rows = rows_ref[:, :, c].reshape(half, width)
        gate_rows_ref[:, :, c] = plain(rows, full_ref[0, 0], NT).reshape(ny, nx, own, units)
        up_rows_ref[:, :, c] = plain(rows, full_ref[0, 1], NT).reshape(ny, nx, own, units)

    @pl.when(mixes)
    def _():
        for j in range(nz):
            hand_copy(ring_index(z, j, nz), j).wait_recv()

    projections(core)
    for i in range(na):
        for j in range(na):
            pair_copy(j, i, True).wait_recv()
    projections(1 - core)
    gate_pre = gate_rows_ref[...].reshape(tokens, units).astype(bf16)
    edge = edge_out.shape[0]
    edge_out[...] = gate_pre[tokens - edge :, :]

    def edge_copy():
        return pltpu.make_async_remote_copy(
            src_ref=edge_out, dst_ref=edge_in, send_sem=edge_send.at[0], recv_sem=edge_recv.at[0],
            device_id=along_z(ring_index(z, 1, nz)), device_id_type=MESH,
        )

    @pl.when(z < nz - 1)
    def _():
        edge_copy().start()

    gate_scr[edge:, :] = gate_pre.astype(f32)
    up_part = up_rows_ref[...].reshape(tokens, units).astype(bf16)

    @pl.when(z > 0)
    def _():
        edge_copy().wait_recv()
        gate_scr[:edge, :] = edge_in[...].astype(f32)

    @pl.when(z == 0)
    def _():
        gate_scr[:edge, :] = jnp.zeros((edge, units), f32)

    count = taps_ref.shape[0]
    conv = jnp.zeros((tokens, units), f32)
    for tap in range(count):
        start = edge - count + 1 + tap
        conv = conv + taps[tap : tap + 1, :] * gate_scr[start : start + tokens, :]
    hidden = (conv / (1.0 + jnp.exp(-conv)) * up_part.astype(f32)).astype(bf16)

    bands = partial.shape[0]
    band = width // bands

    def swap_copy(p):
        return pltpu.make_async_remote_copy(
            src_ref=partial.at[p, :, :, 1 - core], dst_ref=swapped.at[p],
            send_sem=swap_send.at[p], recv_sem=swap_recv.at[p],
            device_id=partner, device_id_type=MESH,
        )

    def first_copy(p, j):
        return pltpu.make_async_remote_copy(
            src_ref=summed.at[p, ring_index(a, j, na)], dst_ref=first.at[p, j],
            send_sem=first_send.at[p, j], recv_sem=first_recv.at[p, j],
            device_id=device(ring_index(a, j, na), b), device_id_type=MESH,
        )

    def last_copy(p, j):
        return pltpu.make_async_remote_copy(
            src_ref=second.at[p, ring_index(b, j, na)], dst_ref=final.at[p, j],
            send_sem=last_send.at[p, j], recv_sem=last_recv.at[p, j],
            device_id=device(a, ring_index(b, j, na)), device_id_type=MESH,
        )

    for p in range(bands):
        product = plain(hidden, full_ref[0, 2, :, p * band : (p + 1) * band]).astype(bf16)
        partial[p] = product.reshape(ny, nx, 2, own, band)
        swap_copy(p).start()
    order = list(range(1, na)) + [0]
    for p in range(bands):
        swap_copy(p).wait_recv()
        for j in order:
            a_to = ring_index(a, j, na)
            for b_to in range(na):
                y_at, x_at = place(a_to, b_to)
                both = partial[p, y_at, x_at, core].astype(f32)
                both = both + swapped[p, y_at, x_at].astype(f32)
                summed[p, a_to, b_to] = both.astype(bf16)
            if j > 0:
                first_copy(p, j).start()
    for p in range(bands):
        for j in range(1, na):
            first_copy(p, j).wait_recv()
        for j in order:
            b_to = ring_index(b, j, na)
            total_rows = summed[p, a, b_to].astype(f32)
            for i in range(1, na):
                total_rows = total_rows + first[p, i, b_to].astype(f32)
            second[p, b_to] = total_rows.astype(bf16)
            if j > 0:
                last_copy(p, j).start()
    for p in range(bands):
        projected = second[p, b].astype(f32)
        for j in range(1, na):
            last_copy(p, j).wait_recv()
        for j in range(1, na):
            projected = projected + final[p, j].astype(f32)
        columns = slice(p * band, (p + 1) * band)
        out_ref[:, columns] = (stream_ref[:, columns] + projected).astype(bf16)

    for j in range(1, ny):
        near_copy(y, j, head_set).wait_send()
        part_copy(j, 1 - head_set).wait_send()

    @pl.when(mixes)
    def _():
        part_copy(0, 1).wait_send()
        for j in range(1, span):
            mid_copy(inner, j).wait_send()
        far_sends("wait_send")
        for j in range(1, nx):
            for to_core in range(2):
                exit_copy(j, to_core).wait_send()
        exit_copy(0, 1 - MIX).wait_send()

    @pl.when(forwards)
    def _():
        if nz > 2 * span:
            pl.semaphore_wait(token_sem, 1)
        near_copy(y, 0, 1).wait_send()
        twin_copy.wait_send()
        finish_copy.wait_send()
        for share in range(2):
            for s in range(n_plus):
                plus_copy(share, s, ring_index(z, -s, nz)).wait_send()
            for s in range(n_minus):
                minus_copy(share, s, ring_index(z, s, nz)).wait_send()
        for j in range(nz):
            hand_copy(ring_index(z, j, nz), j).wait_send()

    for j in range(1, na):
        one_copy(j, False).wait_send()
        for p in range(bands):
            first_copy(p, j).wait_send()
            last_copy(p, j).wait_send()
        for i in range(na):
            two_copy(j, i, False).wait_send()
    for i in range(na):
        for j in range(na):
            pair_copy(j, i, False).wait_send()
    for p in range(bands):
        swap_copy(p).wait_send()

    @pl.when(z < nz - 1)
    def _():
        edge_copy().wait_send()


def layer(*args):
    r, skip, gate = args[0], args[9], args[11]
    nz, ny, nt = lax.axis_size("sp_0"), lax.axis_size("sp_1"), lax.axis_size("tp")
    span = min(4, nz)
    groups = nz // span
    nx = nt // 2
    n = r.shape[0]
    rows, hidden = gate.shape
    units = hidden // ny
    wide = -(-units // 128) * 128
    own, width = skip.shape
    band = width // BANDS
    dma = pltpu.SemaphoreType.DMA
    in_vmem = pl.BlockSpec(memory_space=pltpu.VMEM)
    edge = 16
    return pl.pallas_call(
        functools.partial(layer_kernel, nz, ny, nt, span, len(args)),
        out_shape=jax.ShapeDtypeStruct((own, width), bf16),
        in_specs=[pl.BlockSpec(memory_space=pl.ANY)] * len(args),
        out_specs=in_vmem,
        scratch_shapes=[pltpu.VMEM(arg.shape, arg.dtype) for arg in args]
        + [
            dma((len(args),)),
            pltpu.VMEM((2, 3, units, nz * ny * rows), bf16),
            pltpu.VMEM((ny, 2, n, n), bf16),
            pltpu.VMEM((span, 2, n, n), bf16),
            pltpu.VMEM((groups, 2, n, n), bf16),
            pltpu.VMEM((ny, 3 * rows, wide), bf16),
            pltpu.VMEM((2, ny, 3 * rows, wide), bf16),
            pltpu.VMEM((2, 4, n, n), f32),
            pltpu.VMEM((2, 4, n, n), f32),
            pltpu.VMEM((2, n, n), f32),
            pltpu.VMEM((n, width), bf16),
            pltpu.VMEM((nt, own, width), bf16),
            pltpu.VMEM((nx, own, width), bf16),
            pltpu.VMEM((own, width), f32),
            pltpu.VMEM((ny, nx, 2, own, width), bf16),
            pltpu.VMEM((edge + ny * n, units), f32),
            pltpu.VMEM((edge, units), bf16),
            pltpu.VMEM((edge, units), bf16),
            pltpu.VMEM((BANDS, ny, nx, 2, own, band), bf16),
            pltpu.VMEM((BANDS, ny, nx, own, band), bf16),
            pltpu.VMEM((BANDS, ny, nx, own, band), bf16),
            pltpu.VMEM((BANDS, ny, nx, own, band), bf16),
            pltpu.VMEM((BANDS, nx, own, band), bf16),
            pltpu.VMEM((BANDS, nx, own, band), bf16),
            pltpu.VMEM((ny, nx, 2, own, units), f32),
            pltpu.VMEM((ny, nx, 2, own, units), f32),
            pltpu.SemaphoreType.REGULAR,
            dma((ny,)), dma((ny, 2)), dma((span,)), dma((span,)), dma((groups,)), dma((groups,)),
            dma((ny,)), dma((ny, 2)),
            dma((2, nz)), dma((2, nz)), dma((2, nz)), dma((2, nz)),
            dma((1,)), dma((1,)), dma((1,)), dma((1,)), dma((nz,)), dma((nz,)),
            dma((nx, 2)), dma((nx,)), dma((nx,)), dma((nx,)),
            dma((ny, nx)), dma((ny, nx)), dma((ny, nx)), dma((ny, nx)),
            dma((1,)), dma((1,)), dma((BANDS,)), dma((BANDS,)),
            dma((BANDS, ny)), dma((BANDS, ny)), dma((BANDS, nx)), dma((BANDS, nx)),
        ],
        compiler_params=pltpu.CompilerParams(
            collective_id=0, has_side_effects=True, vmem_limit_bytes=67043328
        ),
        name="layer",
    )(*args)


def body(
    r, k, v, fade, rate, switch, bonus, rescale, leave, skip, scaling, gate, up, taps, down
):
    return layer(
        r, k, v, fade, rate, switch, bonus[None], rescale[None], leave, skip, scaling[None],
        gate, up, taps, down.T,
    )


def solution(mesh):
    sp, tp = mesh.shape["sp"], mesh.shape["tp"]
    ny = COLUMNS
    finer = Mesh(mesh.devices.reshape(sp // ny, ny, tp), SP_TP)
    cut = P(SP, "tp")
    placed = (
        cut, cut, cut, cut, cut, cut, P("tp"), P("tp"), P("tp", None), P(SP_TP, None), P(),
        cut, cut, P(None, "tp"), P("tp", SP),
    )
    return jax.shard_map(
        body, mesh=finer, in_specs=placed, out_specs=P(SP_TP, None), check_vma=False
    )
```

```python
import functools

import jax
import jax.numpy as jnp
from jax import lax
from jax.experimental import pallas as pl
from jax.experimental.pallas import tpu as pltpu
from jax.sharding import Mesh
from jax.sharding import PartitionSpec as P

WIDTH = 64
SP = ("sp_0", "sp_1")
SP_TP = ("sp_0", "sp_1", "tp")
COLUMNS = 4
BANDS = 4
SPLIT = 16
MIX, LATER, LESS = 0, 3, 1
MESH = pl.DeviceIdType.MESH

group_eps = 0.00064
norm_eps = 1e-06
f32 = jnp.float32
bf16 = jnp.bfloat16

NN = (((1,), (0,)), ((), ()))
NT = (((1,), (1,)), ((), ()))
TN = (((0,), (0,)), ((), ()))


def exact(a, b, dims=NN):
    return lax.dot_general(
        a, b, dims, precision=lax.Precision.HIGHEST, preferred_element_type=f32
    )


def plain(a, b, dims=NN):
    return lax.dot_general(a, b, dims, preferred_element_type=f32)


def split(a):
    high = a.astype(bf16)
    return high, (a - high.astype(f32)).astype(bf16)


def fine(a, b, dims=NN):
    (a_dim,), (b_dim,) = dims[0]
    a_high, a_low = split(a)
    b_high, b_low = split(b)
    left = jnp.concatenate([a_high, a_high, a_low], axis=a_dim)
    right = jnp.concatenate([b_high, b_low, b_high], axis=b_dim)
    return plain(left, right, dims)


def left_exact(a, b):
    a = a.astype(bf16)
    return plain(jnp.concatenate([a, a], axis=1), jnp.concatenate(split(b), axis=0))


def right_exact(a, b):
    b = b.astype(bf16)
    return plain(jnp.concatenate(split(a), axis=1), jnp.concatenate([b, b], axis=0))


def iota(shape, dim):
    return lax.broadcasted_iota(jnp.int32, shape, dim)


def ring_index(base, step, size):
    return lax.rem(base + step + size, size)


def head_blocks(n):
    return (iota((n, n), 0) // WIDTH) == (iota((n, n), 1) // WIDTH)


def packed(mapping, state):
    return jnp.concatenate(
        [mapping[:WIDTH] + mapping[WIDTH:], state[:WIDTH] + state[WIDTH:]], axis=0
    ).astype(bf16)


def unpacked_half(half):
    half = half.astype(f32)
    return jnp.where(head_blocks(2 * WIDTH), jnp.concatenate([half, half], axis=0), 0.0)


def unpacked(block):
    return unpacked_half(block[:WIDTH]), unpacked_half(block[WIDTH:])


def compose(earlier, latter):
    both = left_exact(latter[0], jnp.concatenate(earlier, axis=1))
    n = 2 * WIDTH
    return both[:, :n], both[:, n:] + latter[1]


def folded(slots, heads, count, position):
    n = 2 * WIDTH
    eye = jnp.where(iota((n, n), 0) == iota((n, n), 1), 1.0, 0.0)
    before = (eye, jnp.zeros((n, n), f32))
    total = unpacked(slots[0, heads])
    for k in range(1, count):
        hit = position == k
        before = tuple(jnp.where(hit, new, old) for new, old in zip(total, before))
        total = compose(total, unpacked(slots[k, heads]))
    return before, total


def block_inverse(strict, found, first, end):
    n = strict.shape[0]
    row, col = iota((n, n), 0), iota((n, n), 1)
    if found is None:
        found = jnp.where(row == col, 1.0, 0.0) + jnp.where(row // 2 == col // 2, strict, 0.0)
    m = first
    while m < end:
        edge = jnp.where((row // (2 * m) == col // (2 * m)) & (row // m != col // m), strict, 0.0)
        found = found + fine(found, fine(edge, found))
        m *= 2
    return found


def mixer_start(r_ref, k_ref, v_ref, fade_ref, rate_ref):
    r, k, v = r_ref[...].astype(f32), k_ref[...].astype(f32), v_ref[...].astype(f32)
    n = r.shape[0]
    row, col = iota((n, n), 0), iota((n, n), 1)
    ones = jnp.where(head_blocks(n), 1.0, 0.0)
    log_fade = -jax.nn.sigmoid(fade_ref[...]) * 0.6065306597126334
    total_log = left_exact(jnp.where(row >= col, 1.0, 0.0), log_fade)
    length = jnp.sqrt(right_exact(k * k, ones))
    unit = k / jnp.maximum(length, 1.0)
    amount = unit * jax.nn.sigmoid(rate_ref[...])
    kept = jnp.exp(total_log)
    grown = jnp.exp(-total_log)
    erase = -unit * jnp.exp(total_log - log_fade)
    read = r * kept
    amount_grown, key_grown = amount * grown, k * grown
    last = kept[n - 1 :, :]
    right = jnp.concatenate([amount_grown, key_grown], axis=0)
    heads = []
    for h in range(n // WIDTH):
        mine = col // WIDTH == h
        erase_h = jnp.where(mine, erase, 0.0)
        read_h = jnp.where(mine, read, 0.0)
        grams = fine(jnp.concatenate([erase_h, read_h], axis=0), right, NT)
        within = jnp.where(row > col, grams[:n, :n], 0.0)
        heads.append((erase_h, grams, within, block_inverse(within, None, 2, SPLIT)))
    return v, read, last, amount_grown, key_grown, heads


def mixer_end(v, read, last, amount_grown, key_grown, heads):
    n = v.shape[0]
    row, col = iota((n, n), 0), iota((n, n), 1)
    strict, lower = row > col, row >= col
    maps = jnp.zeros((n, n), f32)
    values = jnp.zeros((n, n), f32)
    probe, local_out = read, jnp.zeros((n, n), f32)
    for h, (erase_h, grams, within, inverse) in enumerate(heads):
        value_h = jnp.where(col // WIDTH == h, v, 0.0)
        inverse = block_inverse(within, inverse, SPLIT, n)
        pushed = fine(jnp.where(strict, grams[:n, n:], 0.0), value_h)
        solved = fine(inverse, jnp.concatenate([erase_h, pushed], axis=1))
        shown = fine(jnp.where(lower, grams[n:, :n], 0.0), solved)
        local_out = local_out + shown[:, n:]
        local_out = local_out + fine(jnp.where(lower, grams[n:, n:], 0.0), value_h)
        probe = probe + shown[:, :n]
        maps = maps + solved[:, :n]
        values = values + solved[:, n:]
    same = head_blocks(n)
    amount_end, key_end = amount_grown * last, key_grown * last
    mapping = jnp.where(row == col, last, 0.0) + jnp.where(same, fine(amount_end, maps, TN), 0.0)
    state = jnp.where(same, fine(amount_end, values, TN) + fine(key_end, v, TN), 0.0)
    return mapping, state, probe, local_out


def layer_kernel(
    nz, ny, nt, span, inputs, *refs,
):
    given, out_ref, held = refs[:inputs], refs[inputs], refs[inputs + 1 : 2 * inputs + 1]
    load_sem, rest = refs[2 * inputs + 1], refs[2 * inputs + 2 :]
    (
        r_ref, k_ref, v_ref, fade_ref, rate_ref, switch_ref, bonus_ref, rescale_ref,
        exit_ref, skip_ref, scaling_ref, gate_ref, up_ref, taps_ref, down_ref,
    ) = held
    loads = [
        pltpu.make_async_copy(source, target, load_sem.at[i])
        for i, (source, target) in enumerate(zip(given, held))
    ]
    first_loads, second_loads = [3, 1, 4, 0, 2], [11, 12, 14]
    last_loads = [i for i in range(inputs) if i not in first_loads + second_loads]
    for i in first_loads + second_loads + last_loads:
        loads[i].start()
    (
    full_ref, near, mid, far, pieces, parts, finish_ref, before_ref, carry_ref, exit_both,
    sent, landed, stream_ref, rows_ref, gate_scr, edge_out, edge_in, partial, swapped, summed,
    first, second, final, gate_rows_ref, up_rows_ref,
    token_sem, near_send, near_recv, mid_send, mid_recv, far_send, far_recv, part_send, part_recv,
    plus_send, plus_recv, minus_send, minus_recv,
    finish_send, finish_recv, twin_send, twin_recv, hand_send, hand_recv,
    exit_send, exit_recv, one_send, one_recv, two_send, two_recv, pair_send, pair_recv,
    edge_send, edge_recv, swap_send, swap_recv, first_send, first_recv, last_send, last_recv,
    ) = rest
    z, y, t = lax.axis_index("sp_0"), lax.axis_index("sp_1"), lax.axis_index("tp")
    nx = nt // 2
    x, core = t // 2, lax.rem(t, 2)
    groups = nz // span
    inner, outer = lax.rem(z, span), z // span
    n = 2 * WIDTH
    units = full_ref.shape[2]
    rows = gate_ref.shape[0]

    def along_y(j):
        return {"sp_1": ring_index(y, j, ny)}

    def along_z(to):
        return {"sp_0": to}

    mixes = core == MIX
    forwards = core == 1 - MIX
    head_set = jnp.where(mixes, 0, 1)
    chip = t - core
    mate = chip + 1 - core
    mixer_at, ring_at = chip + MIX, chip + 1 - MIX

    barrier = pltpu.get_barrier_semaphore()
    for j in range(1, ny):
        for to in (t, mate):
            pl.semaphore_signal(
                barrier, inc=1, device_id={"sp_1": ring_index(y, j, ny), "tp": to},
                device_id_type=MESH,
            )
    reach = sorted({j % nz for j in range(-span, span + 1)} - {0})
    for j in reach:
        pl.semaphore_signal(
            barrier, inc=1, device_id=along_z(ring_index(z, j, nz)), device_id_type=MESH
        )
    for j in range(1, nt):
        pl.semaphore_signal(
            barrier, inc=1, device_id={"tp": ring_index(t, j, nt)}, device_id_type=MESH
        )

    for i in first_loads:
        loads[i].wait()
    begun = mixer_start(r_ref, k_ref, v_ref, fade_ref, rate_ref)

    for i in second_loads:
        loads[i].wait()
    stacked = jnp.concatenate([gate_ref[...], up_ref[...], down_ref[...]], axis=0)
    wide = pieces.shape[2]
    tall = stacked.shape[1]
    for part in range(ny):
        at, to = iota((tall, wide), 0), iota((tall, wide), 1)
        pick = jnp.where((at == to + part * units) & (to < units), 1.0, 0.0).astype(bf16)
        pieces[part] = plain(stacked, pick).astype(bf16)

    for i in last_loads:
        loads[i].wait()
    pl.semaphore_wait(barrier, 2 * (ny - 1) + len(reach) + nt - 1)
    if nz > 2 * span:
        pl.semaphore_signal(
            token_sem, inc=1, device_id=along_z(ring_index(z, -span, nz)), device_id_type=MESH
        )

    def near_copy(source, j, heads):
        return pltpu.make_async_remote_copy(
            src_ref=near.at[source, heads], dst_ref=near.at[source, heads],
            send_sem=near_send.at[j], recv_sem=near_recv.at[j, heads],
            device_id={"sp_1": ring_index(y, j, ny), "tp": mixer_at}, device_id_type=MESH,
        )

    def part_copy(j, share):
        to = ring_index(y, j, ny)
        return pltpu.make_async_remote_copy(
            src_ref=pieces.at[to], dst_ref=parts.at[share, y],
            send_sem=part_send.at[j], recv_sem=part_recv.at[j, share],
            device_id={"sp_1": to, "tp": ring_at}, device_id_type=MESH,
        )

    def part_arrival(j, share):
        source = ring_index(y, -j, ny)
        return pltpu.make_async_remote_copy(
            src_ref=pieces.at[source], dst_ref=parts.at[share, source],
            send_sem=part_send.at[j], recv_sem=part_recv.at[j, share],
            device_id={"sp_1": source, "tp": ring_at}, device_id_type=MESH,
        )

    share = 1 - head_set
    for j in range(1, ny):
        part_copy(j, share).start()

    @pl.when(mixes)
    def _():
        part_copy(0, 1).start()

    @pl.when(forwards)
    def _():
        parts[0, y] = pieces[y]

    twin_copy = pltpu.make_async_remote_copy(
        src_ref=exit_ref, dst_ref=exit_both, send_sem=twin_send.at[0], recv_sem=twin_recv.at[0],
        device_id={"tp": mate}, device_id_type=MESH,
    )

    @pl.when(forwards)
    def _():
        twin_copy.start()

    mapping, state, probe, local_out = mixer_end(*begun)
    near[y, head_set] = packed(mapping, state)
    for j in range(1, ny):
        near_copy(y, j, head_set).start()

    @pl.when(forwards)
    def _():
        near_copy(y, 0, 1).start()

    ones = jnp.where(head_blocks(n), 1.0, 0.0)
    value, switch = v_ref[...].astype(f32), switch_ref[...].astype(f32)
    bonus = right_exact(r_ref[...].astype(f32) * k_ref[...].astype(f32) * bonus_ref[...], ones)
    finish_ref[head_set, 0] = probe
    finish_ref[head_set, 1] = local_out
    finish_ref[head_set, 2] = rescale_ref[...] * switch
    finish_ref[head_set, 3] = bonus * value * switch
    finish_copy = pltpu.make_async_remote_copy(
        src_ref=finish_ref.at[1], dst_ref=finish_ref.at[1],
        send_sem=finish_send.at[0], recv_sem=finish_recv.at[0],
        device_id={"tp": mate}, device_id_type=MESH,
    )

    @pl.when(forwards)
    def _():
        finish_copy.start()

    depth = ny * rows

    def piece(share, at):
        return full_ref.at[share, :, :, pl.ds(pl.multiple_of(at * depth, depth), depth)]

    def plus_copy(share, s, at):
        ref = piece(share, at)
        return pltpu.make_async_remote_copy(
            src_ref=ref, dst_ref=ref,
            send_sem=plus_send.at[share, s], recv_sem=plus_recv.at[share, s],
            device_id=along_z(ring_index(z, 1, nz)), device_id_type=MESH,
        )

    def minus_copy(share, s, at):
        ref = piece(share, at)
        return pltpu.make_async_remote_copy(
            src_ref=ref, dst_ref=ref,
            send_sem=minus_send.at[share, s], recv_sem=minus_recv.at[share, s],
            device_id=along_z(ring_index(z, -1, nz)), device_id_type=MESH,
        )

    def hand_copy(at, j):
        return pltpu.make_async_remote_copy(
            src_ref=piece(1, at), dst_ref=piece(0, at),
            send_sem=hand_send.at[j], recv_sem=hand_recv.at[j],
            device_id={"tp": mate}, device_id_type=MESH,
        )

    n_plus = max(1, nz // 2 - LESS) if nz > 2 else 1
    n_minus = nz - 1 - n_plus
    steps = max(n_plus, n_minus) + 1

    def ring_step(s):
        for share in range(2):
            after, ahead = ring_index(z, -s, nz), ring_index(z, s, nz)
            if s > 0 and s <= n_plus:
                plus_copy(share, s - 1, after).wait_recv()
            if s < n_plus:
                plus_copy(share, s, after).start()
            if s > 0 and s <= n_minus:
                minus_copy(share, s - 1, ahead).wait_recv()
            if s < n_minus:
                minus_copy(share, s, ahead).start()
            if share == 1:
                if s <= n_plus:
                    hand_copy(after, (nz - s) % nz).start()
                if s > 0 and s <= n_minus:
                    hand_copy(ahead, s).start()

    @pl.when(forwards)
    def _():
        for j in range(1, ny):
            for share in range(2):
                part_arrival(j, share).wait_recv()
        part_copy(0, 1).wait_recv()
        square = jnp.where(iota((units, wide), 0) == iota((units, wide), 1), 1.0, 0.0).astype(bf16)
        for share in range(2):
            for c in range(3):
                tallest = jnp.concatenate(
                    [parts[share, part, c * rows : (c + 1) * rows, :] for part in range(ny)], axis=0
                )
                block = plain(square, tallest, NT).astype(bf16)
                full_ref[share, c, :, pl.ds(pl.multiple_of(z * depth, depth), depth)] = block
        for s in range(max(0, steps - LATER)):
            ring_step(s)

    def later_ring_steps(first, end):
        todo = list(range(max(0, steps - LATER), steps))[first:end]
        if todo:
            @pl.when(forwards)
            def _():
                for s in todo:
                    ring_step(s)

    def mid_copy(source, j):
        to = z - inner + ring_index(inner, j, span)
        return pltpu.make_async_remote_copy(
            src_ref=mid.at[source], dst_ref=mid.at[source],
            send_sem=mid_send.at[j], recv_sem=mid_recv.at[j],
            device_id=along_z(to), device_id_type=MESH,
        )

    def far_copy(source, d, to, states_only):
        ref = far.at[source, 1] if states_only else far.at[source]
        return pltpu.make_async_remote_copy(
            src_ref=ref, dst_ref=ref, send_sem=far_send.at[d], recv_sem=far_recv.at[d],
            device_id=along_z(to), device_id_type=MESH,
        )

    def far_sends(action):
        for d in range(1, groups):
            to = lax.rem(z + d * span, nz)

            @pl.when(outer == 0)
            def _():
                getattr(far_copy(0, d, to, True), action)()

            @pl.when((outer > 0) & (outer + d < groups))
            def _():
                getattr(far_copy(outer, d, to, False), action)()

    def exit_copy(j, to_core):
        to = 2 * ring_index(x, j, nx) + to_core
        return pltpu.make_async_remote_copy(
            src_ref=sent.at[to], dst_ref=landed.at[j],
            send_sem=exit_send.at[j, to_core], recv_sem=exit_recv.at[j],
            device_id={"tp": to}, device_id_type=MESH,
        )

    own = n // nt
    width = exit_ref.shape[1]

    @pl.when(mixes)
    def _():
        for j in range(1, ny):
            for heads in range(2):
                near_copy(ring_index(y, -j, ny), j, heads).wait_recv()
        near_copy(y, 0, 1).wait_recv()
        totals = []
        for heads in range(2):
            before, total = folded(near, heads, ny, y)
            before_ref[heads, 0], before_ref[heads, 1] = before
            totals.append(packed(*total))
        for heads in range(2):
            mid[inner, heads] = totals[heads]
        for j in range(1, span):
            mid_copy(inner, j).start()
        for j in range(1, span):
            mid_copy(ring_index(inner, -j, span), j).wait_recv()
        totals = []
        for heads in range(2):
            before, total = folded(mid, heads, span, inner)
            before_ref[heads, 2], before_ref[heads, 3] = before
            totals.append(packed(*total))
        far[outer, 0] = jnp.concatenate([part[:WIDTH] for part in totals], axis=0)
        far[outer, 1] = jnp.concatenate([part[WIDTH:] for part in totals], axis=0)
        if nz > 2 * span:
            pl.semaphore_wait(token_sem, 1)
        far_sends("start")
        carry_ref[...] = jnp.zeros((2, n, n), f32)
        finish_copy.wait_recv()
        twin_copy.wait_recv()
        for heads in range(2):
            map_y, state_y, map_z, state_z = (before_ref[heads, k] for k in range(4))
            shown = fine(map_y, jnp.concatenate([map_z, state_z], axis=1))
            entry = jnp.concatenate([shown[:, :n], shown[:, n:] + state_y], axis=1)
            seen = fine(finish_ref[heads, 0], entry)
            finish_ref[heads, 0] = seen[:, :n]
            finish_ref[heads, 1] = finish_ref[heads, 1] + seen[:, n:]
        for g in range(groups - 1):
            @pl.when(outer > g)
            def _():
                for d in range(1, groups):
                    @pl.when(outer - g == d)
                    def _():
                        far_copy(g, d, lax.rem(z + d * span, nz), g == 0).wait_recv()
                for heads in range(2):
                    half = slice(heads * WIDTH, (heads + 1) * WIDTH)
                    state = unpacked_half(far[g, 1, half])
                    if g > 0:
                        state = state + left_exact(unpacked_half(far[g, 0, half]), carry_ref[heads])
                    carry_ref[heads] = state
        mixed = []
        for heads in range(2):
            closing = finish_ref[heads, 1] + fine(finish_ref[heads, 0], carry_ref[heads])
            centred = closing - right_exact(closing, ones) * (1.0 / WIDTH)
            spread = right_exact(centred * centred, ones) * (1.0 / WIDTH)
            rescaled = centred * lax.rsqrt(spread + group_eps) * finish_ref[heads, 2]
            mixed.append((rescaled + finish_ref[heads, 3]).astype(bf16))
        product = plain(
            jnp.concatenate(mixed, axis=1), jnp.concatenate([exit_ref[...], exit_both[...]], axis=0)
        )
        sent[...] = product.astype(bf16).reshape(nt, own, width)
        for j in range(1, nx):
            for to_core in range(2):
                exit_copy(j, to_core).start()
        exit_copy(0, 1 - MIX).start()

    stream = skip_ref[...].astype(f32)
    for j in range(1, nx):
        exit_copy(j, core).wait_recv()

    @pl.when(mixes)
    def _():
        landed[0] = sent[t]

    @pl.when(forwards)
    def _():
        exit_copy(0, 1 - MIX).wait_recv()

    for j in range(nx):
        stream = stream + landed[j].astype(f32)
    stream_ref[...] = stream
    mean = jnp.mean(stream * stream, axis=-1, keepdims=True)
    rows_ref[y, x, core] = (stream * lax.rsqrt(mean + norm_eps) * scaling_ref[...]).astype(bf16)

    across = 1 - core
    na = ny
    a, b = y * across + x * core, x * across + y * core

    def place(a_to, b_to):
        return a_to * across + b_to * core, b_to * across + a_to * core

    def device(a_to, b_to):
        y_to, x_to = place(a_to, b_to)
        return {"sp_1": y_to, "tp": 2 * x_to + core}

    def slot(j, i):
        y_at, x_at = place(ring_index(a, -j, na), ring_index(b, -i, na))
        return rows_ref.at[y_at, x_at, core]

    def one_copy(j, arriving):
        ref = slot(0, j if arriving else 0)
        return pltpu.make_async_remote_copy(
            src_ref=ref, dst_ref=ref, send_sem=one_send.at[j], recv_sem=one_recv.at[j],
            device_id=device(a, ring_index(b, j, na)), device_id_type=MESH,
        )

    def two_copy(j, i, arriving):
        ref = slot(j if arriving else 0, i)
        return pltpu.make_async_remote_copy(
            src_ref=ref, dst_ref=ref, send_sem=two_send.at[j, i], recv_sem=two_recv.at[j, i],
            device_id=device(ring_index(a, j, na), b), device_id_type=MESH,
        )

    partner = {"tp": mate}

    def pair_copy(j, i, arriving):
        if arriving:
            y_at, x_at = place(ring_index(a, -i, na), ring_index(b, -j, na))
            ref = rows_ref.at[y_at, x_at, 1 - core]
        else:
            ref = slot(j, i)
        return pltpu.make_async_remote_copy(
            src_ref=ref, dst_ref=ref, send_sem=pair_send.at[j, i], recv_sem=pair_recv.at[j, i],
            device_id=partner, device_id_type=MESH,
        )

    for j in range(1, na):
        one_copy(j, False).start()
    for j in range(1, na):
        two_copy(j, 0, False).start()
    pair_copy(0, 0, False).start()
    units_at = iota((taps_ref.shape[1], units), 0) == iota((taps_ref.shape[1], units), 1) + y * units
    taps = exact(taps_ref[...], jnp.where(units_at, 1.0, 0.0))
    later_ring_steps(0, 1)
    for i in range(1, na):
        one_copy(i, True).wait_recv()
        for j in range(1, na):
            two_copy(j, i, False).start()
        pair_copy(0, i, False).start()
    later_ring_steps(1, LATER)
    for i in range(na):
        for j in range(1, na):
            two_copy(j, i, True).wait_recv()
            pair_copy(j, i, False).start()
    tokens = na * n
    half = tokens // 2

    def projections(c):
        rows = rows_ref[:, :, c].reshape(half, width)
        gate_rows_ref[:, :, c] = plain(rows, full_ref[0, 0], NT).reshape(ny, nx, own, units)
        up_rows_ref[:, :, c] = plain(rows, full_ref[0, 1], NT).reshape(ny, nx, own, units)

    @pl.when(mixes)
    def _():
        for j in range(nz):
            hand_copy(ring_index(z, j, nz), j).wait_recv()

    projections(core)
    for i in range(na):
        for j in range(na):
            pair_copy(j, i, True).wait_recv()
    projections(1 - core)
    gate_pre = gate_rows_ref[...].reshape(tokens, units).astype(bf16)
    edge = edge_out.shape[0]
    edge_out[...] = gate_pre[tokens - edge :, :]

    def edge_copy():
        return pltpu.make_async_remote_copy(
            src_ref=edge_out, dst_ref=edge_in, send_sem=edge_send.at[0], recv_sem=edge_recv.at[0],
            device_id=along_z(ring_index(z, 1, nz)), device_id_type=MESH,
        )

    @pl.when(z < nz - 1)
    def _():
        edge_copy().start()

    gate_scr[edge:, :] = gate_pre.astype(f32)
    up_part = up_rows_ref[...].reshape(tokens, units).astype(bf16)

    @pl.when(z > 0)
    def _():
        edge_copy().wait_recv()
        gate_scr[:edge, :] = edge_in[...].astype(f32)

    @pl.when(z == 0)
    def _():
        gate_scr[:edge, :] = jnp.zeros((edge, units), f32)

    count = taps_ref.shape[0]
    conv = jnp.zeros((tokens, units), f32)
    for tap in range(count):
        start = edge - count + 1 + tap
        conv = conv + taps[tap : tap + 1, :] * gate_scr[start : start + tokens, :]
    hidden = (conv / (1.0 + jnp.exp(-conv)) * up_part.astype(f32)).astype(bf16)

    bands = partial.shape[0]
    band = width // bands

    def swap_copy(p):
        return pltpu.make_async_remote_copy(
            src_ref=partial.at[p, :, :, 1 - core], dst_ref=swapped.at[p],
            send_sem=swap_send.at[p], recv_sem=swap_recv.at[p],
            device_id=partner, device_id_type=MESH,
        )

    def first_copy(p, j):
        return pltpu.make_async_remote_copy(
            src_ref=summed.at[p, ring_index(a, j, na)], dst_ref=first.at[p, j],
            send_sem=first_send.at[p, j], recv_sem=first_recv.at[p, j],
            device_id=device(ring_index(a, j, na), b), device_id_type=MESH,
        )

    def last_copy(p, j):
        return pltpu.make_async_remote_copy(
            src_ref=second.at[p, ring_index(b, j, na)], dst_ref=final.at[p, j],
            send_sem=last_send.at[p, j], recv_sem=last_recv.at[p, j],
            device_id=device(a, ring_index(b, j, na)), device_id_type=MESH,
        )

    for p in range(bands):
        product = plain(hidden, full_ref[0, 2, :, p * band : (p + 1) * band]).astype(bf16)
        partial[p] = product.reshape(ny, nx, 2, own, band)
        swap_copy(p).start()
    order = list(range(1, na)) + [0]
    for p in range(bands):
        swap_copy(p).wait_recv()
        for j in order:
            a_to = ring_index(a, j, na)
            for b_to in range(na):
                y_at, x_at = place(a_to, b_to)
                both = partial[p, y_at, x_at, core].astype(f32)
                both = both + swapped[p, y_at, x_at].astype(f32)
                summed[p, a_to, b_to] = both.astype(bf16)
            if j > 0:
                first_copy(p, j).start()
    for p in range(bands):
        for j in range(1, na):
            first_copy(p, j).wait_recv()
        for j in order:
            b_to = ring_index(b, j, na)
            total_rows = summed[p, a, b_to].astype(f32)
            for i in range(1, na):
                total_rows = total_rows + first[p, i, b_to].astype(f32)
            second[p, b_to] = total_rows.astype(bf16)
            if j > 0:
                last_copy(p, j).start()
    for p in range(bands):
        projected = second[p, b].astype(f32)
        for j in range(1, na):
            last_copy(p, j).wait_recv()
        for j in range(1, na):
            projected = projected + final[p, j].astype(f32)
        columns = slice(p * band, (p + 1) * band)
        out_ref[:, columns] = (stream_ref[:, columns] + projected).astype(bf16)

    for j in range(1, ny):
        near_copy(y, j, head_set).wait_send()
        part_copy(j, 1 - head_set).wait_send()

    @pl.when(mixes)
    def _():
        part_copy(0, 1).wait_send()
        for j in range(1, span):
            mid_copy(inner, j).wait_send()
        far_sends("wait_send")
        for j in range(1, nx):
            for to_core in range(2):
                exit_copy(j, to_core).wait_send()
        exit_copy(0, 1 - MIX).wait_send()

    @pl.when(forwards)
    def _():
        if nz > 2 * span:
            pl.semaphore_wait(token_sem, 1)
        near_copy(y, 0, 1).wait_send()
        twin_copy.wait_send()
        finish_copy.wait_send()
        for share in range(2):
            for s in range(n_plus):
                plus_copy(share, s, ring_index(z, -s, nz)).wait_send()
            for s in range(n_minus):
                minus_copy(share, s, ring_index(z, s, nz)).wait_send()
        for j in range(nz):
            hand_copy(ring_index(z, j, nz), j).wait_send()

    for j in range(1, na):
        one_copy(j, False).wait_send()
        for p in range(bands):
            first_copy(p, j).wait_send()
            last_copy(p, j).wait_send()
        for i in range(na):
            two_copy(j, i, False).wait_send()
    for i in range(na):
        for j in range(na):
            pair_copy(j, i, False).wait_send()
    for p in range(bands):
        swap_copy(p).wait_send()

    @pl.when(z < nz - 1)
    def _():
        edge_copy().wait_send()


def layer(*args):
    r, skip, gate = args[0], args[9], args[11]
    nz, ny, nt = lax.axis_size("sp_0"), lax.axis_size("sp_1"), lax.axis_size("tp")
    span = min(4, nz)
    groups = nz // span
    nx = nt // 2
    n = r.shape[0]
    rows, hidden = gate.shape
    units = hidden // ny
    wide = -(-units // 128) * 128
    own, width = skip.shape
    band = width // BANDS
    dma = pltpu.SemaphoreType.DMA
    in_vmem = pl.BlockSpec(memory_space=pltpu.VMEM)
    edge = 16
    return pl.pallas_call(
        functools.partial(layer_kernel, nz, ny, nt, span, len(args)),
        out_shape=jax.ShapeDtypeStruct((own, width), bf16),
        in_specs=[pl.BlockSpec(memory_space=pl.ANY)] * len(args),
        out_specs=in_vmem,
        scratch_shapes=[pltpu.VMEM(arg.shape, arg.dtype) for arg in args]
        + [
            dma((len(args),)),
            pltpu.VMEM((2, 3, units, nz * ny * rows), bf16),
            pltpu.VMEM((ny, 2, n, n), bf16),
            pltpu.VMEM((span, 2, n, n), bf16),
            pltpu.VMEM((groups, 2, n, n), bf16),
            pltpu.VMEM((ny, 3 * rows, wide), bf16),
            pltpu.VMEM((2, ny, 3 * rows, wide), bf16),
            pltpu.VMEM((2, 4, n, n), f32),
            pltpu.VMEM((2, 4, n, n), f32),
            pltpu.VMEM((2, n, n), f32),
            pltpu.VMEM((n, width), bf16),
            pltpu.VMEM((nt, own, width), bf16),
            pltpu.VMEM((nx, own, width), bf16),
            pltpu.VMEM((own, width), f32),
            pltpu.VMEM((ny, nx, 2, own, width), bf16),
            pltpu.VMEM((edge + ny * n, units), f32),
            pltpu.VMEM((edge, units), bf16),
            pltpu.VMEM((edge, units), bf16),
            pltpu.VMEM((BANDS, ny, nx, 2, own, band), bf16),
            pltpu.VMEM((BANDS, ny, nx, own, band), bf16),
            pltpu.VMEM((BANDS, ny, nx, own, band), bf16),
            pltpu.VMEM((BANDS, ny, nx, own, band), bf16),
            pltpu.VMEM((BANDS, nx, own, band), bf16),
            pltpu.VMEM((BANDS, nx, own, band), bf16),
            pltpu.VMEM((ny, nx, 2, own, units), f32),
            pltpu.VMEM((ny, nx, 2, own, units), f32),
            pltpu.SemaphoreType.REGULAR,
            dma((ny,)), dma((ny, 2)), dma((span,)), dma((span,)), dma((groups,)), dma((groups,)),
            dma((ny,)), dma((ny, 2)),
            dma((2, nz)), dma((2, nz)), dma((2, nz)), dma((2, nz)),
            dma((1,)), dma((1,)), dma((1,)), dma((1,)), dma((nz,)), dma((nz,)),
            dma((nx, 2)), dma((nx,)), dma((nx,)), dma((nx,)),
            dma((ny, nx)), dma((ny, nx)), dma((ny, nx)), dma((ny, nx)),
            dma((1,)), dma((1,)), dma((BANDS,)), dma((BANDS,)),
            dma((BANDS, ny)), dma((BANDS, ny)), dma((BANDS, nx)), dma((BANDS, nx)),
        ],
        compiler_params=pltpu.CompilerParams(
            collective_id=0, has_side_effects=True, vmem_limit_bytes=67043328
        ),
        name="layer",
    )(*args)


def body(
    r, k, v, fade, rate, switch, bonus, rescale, leave, skip, scaling, gate, up, taps, down
):
    return layer(
        r, k, v, fade, rate, switch, bonus[None], rescale[None], leave, skip, scaling[None],
        gate, up, taps, down.T,
    )


def solution(mesh):
    sp, tp = mesh.shape["sp"], mesh.shape["tp"]
    ny = COLUMNS
    finer = Mesh(mesh.devices.reshape(sp // ny, ny, tp), SP_TP)
    cut = P(SP, "tp")
    placed = (
        cut, cut, cut, cut, cut, cut, P("tp"), P("tp"), P("tp", None), P(SP_TP, None), P(),
        cut, cut, P(None, "tp"), P("tp", SP),
    )
    return jax.shard_map(
        body, mesh=finer, in_specs=placed, out_specs=P(SP_TP, None), check_vma=False
    )
```
